256 devices in a mesh: ep: 128 (over z, y, x_hi, core), tp: 2 (over x_lo).
Axes of the slice: x: 4 (x_hi: 2, x_lo: 2; x = x_hi * 2 + x_lo), y: 4, z: 8, core: 2. Of those that a mesh axis runs over, the one named last changes fastest.
Arguments:
- tokens: bfloat16 [1536, 2048], P('ep'), may hold values from -6 to 6
- norm_gain: float32 [2048], replicated, may hold values from 0.1 to 1.9
- w_query: bfloat16 [2048, 768], P(None, 'tp'), may hold values from -0.125 to 0.125
- w_key: bfloat16 [2048, 768], P(None, 'tp'), may hold values from -0.125 to 0.125
- w_value: bfloat16 [2048, 768], P(None, 'tp'), may hold values from -0.125 to 0.125
- w_outgate: bfloat16 [2048, 768], P(None, 'tp'), may hold values from -0.125 to 0.125
- w_input_gate: bfloat16 [2048, 4], replicated, may hold values from -0.125 to 0.125
- w_forget_gate: bfloat16 [2048, 4], replicated, may hold values from -0.125 to 0.125
- forget_bias: float32 [4], replicated, may hold values from -1 to 4
- head_gain: float32 [768], replicated, may hold values from 0.1 to 1.9
- w_output: bfloat16 [768, 2048], P('tp'), may hold values from -0.21875 to 0.21875
- memory: float32 [1536, 4, 192, 192], P('ep', 'tp'), may hold values from -2 to 2
- normalizer: float32 [1536, 4, 192], P('ep', 'tp'), may hold values from -2 to 2
- stabilizer: float32 [1536, 4], P('ep', 'tp'), may hold values from -2 to 2
- ffn_gain: float32 [2048], replicated, may hold values from 0.1 to 1.9
- route_ids: int32 [1536, 4], P('ep'), may hold values from 0 to 127, all different within a row; in each aligned block of 12 rows (0 to 11, 12 to 23, ...) at most 2 rows name the same one
- route_probs: float32 [1536, 4], P('ep'), may hold values from 0.05 to 1
- expert_gate: bfloat16 [128, 2048, 1024], P('ep', None, 'tp'), may hold values from -0.125 to 0.125
- expert_up: bfloat16 [128, 2048, 1024], P('ep', None, 'tp'), may hold values from -0.125 to 0.125
- expert_down: bfloat16 [128, 1024, 2048], P('ep', 'tp'), may hold values from -0.1875 to 0.1875
Outputs:
- next_tokens: bfloat16 [1536, 2048], P('ep')
- new_memory: float32 [1536, 4, 192, 192], P('ep', 'tp')
- new_normalizer: float32 [1536, 4, 192], P('ep', 'tp')
- new_stabilizer: float32 [1536, 4], P('ep', 'tp')
The draws below stay inside these ranges and needn't reach their ends.
Inputs may be any that keep to these rules, and one draw needn't show every extreme that they name: `route_ids`: in each aligned block of 12 rows (the rows of one index of ep), no expert appears more than 2 times among the block's routes, and some expert appears exactly 2 times; the 4 experts of a row are different.
All inputs are finite; a program needn't handle non-finite values.
Results may differ from the reference program's by a relative error of at most 0.015.
Values may be sent and summed in bfloat16 or wider, within the bound.
A program may use at most 128 MiB of HBM per device.

```python
import math
import jax
import jax.numpy as jnp
import numpy as np
from jax import lax

D = 2048
HEADS = 4
DH = 192
FFE = 1024
TOPK = 4
B_DEV = 12
INNER = 768
EXPERTS = 128
BATCH = 1536
CAP = 2
N_EP = 128
N_TP = 2


def block_levels(stream_key, dims, cuts, smallest, high):
    def one(axis_at, blocks):
        steps = jax.random.uniform(jax.random.fold_in(jax.random.fold_in(stream_key, 6), axis_at), (blocks,), jnp.float32, smallest / len(cuts), high / len(cuts))
        return jnp.repeat(jnp.exp(steps), dims[axis_at] // blocks).reshape((-1,) + (1,) * (len(dims) - axis_at - 1))

    loudness = one(*cuts[0])
    for cut in cuts[1:]:
        loudness = loudness * one(*cut)
    return loudness


def shared_out(key, own, number, rows, number_of, top, reach, slope):
    sequence = jax.random.permutation(key, number_of)
    heavy_load, ordinary = portions_of(number_of, rows * top, reach, slope, True), portions_of(number_of, rows * top, reach, slope, False)
    places = jnp.arange(number_of)

    def named(lengths, rotation):
        used = int((lengths > 0).sum())
        fixed = max(1, used // 4)
        moved = fixed + (places - fixed + rotation * (used - fixed)) % max(1, number_of - fixed)
        return jnp.zeros((number_of,), jnp.int32).at[sequence[jnp.where(places < fixed, places, moved)]].set(jnp.asarray(lengths, jnp.int32))

    lengths = jnp.where(number % 4 == 0, named(heavy_load, number // 4), named(ordinary, number - number // 4 - 1))
    mixed = jax.random.permutation(jax.random.fold_in(own, 3), number_of)
    source_of, taker = mixed[0:number_of // 2 * 2:2], mixed[1:number_of // 2 * 2:2]
    margin = jnp.minimum(lengths[source_of] - 1, reach - lengths[taker]) // 2
    margin = jnp.where((source_of == sequence[0]) | (taker == sequence[0]) | (lengths[taker] == 0), 0, jnp.maximum(margin, 0))
    moved = jax.random.randint(jax.random.fold_in(own, 4), (number_of // 2,), 0, 1 << 20) % (margin + 1)
    lengths = lengths.at[source_of].add(-moved).at[taker].add(moved)
    items = jnp.searchsorted(jnp.cumsum(lengths), jnp.arange(rows * top), side="right").astype(jnp.int32)
    table = items.reshape(top, rows).T
    table = table[jax.random.permutation(jax.random.fold_in(own, 1), rows)]
    rotation = jax.random.randint(jax.random.fold_in(own, 2), (rows, 1), 0, top)
    return jnp.take_along_axis(table, (jnp.arange(top)[None, :] + rotation) % top, axis=1)


def portions_of(number_of, total, reach, skew, full):
    weights = [(1 << 20) // math.isqrt(rank ** skew) + 1 for rank in range(1, number_of + 1)]
    largest = reach if full else min(reach, max(-(-total // number_of), total * weights[0] // sum(weights)))
    least = 1 if total - largest >= number_of - 1 else 0
    holding, spare = [largest] + [least] * (number_of - 1), total - largest - least * (number_of - 1)
    while spare > 0:
        free = [i for i in range(1, number_of) if holding[i] < largest] or [i for i in range(1, number_of) if holding[i] < reach]
        mass, budget = sum([weights[i] for i in free]), spare
        for i in free:
            more = min(reach - holding[i], max(1, budget * weights[i] // mass), spare)
            holding[i] = holding[i] + more
            spare = spare - more
    return np.array(holding)


def gaussian(stream_key, shape, spread, reach, shards=(), kind=jnp.bfloat16):
    factor_of = block_levels(stream_key, shape, shards, -0.22, 0.18) if shards else 1.0
    drawn = jax.random.normal(stream_key, shape, jnp.float32) * spread * factor_of
    return jnp.minimum(jnp.maximum(drawn, -reach), reach).astype(kind)


def setup_inputs(seed: int = 0) -> dict:
    keys = jax.random.split(jax.random.key(seed), 21)
    tokens = gaussian(keys[0], (BATCH, D), 1.0, 6.0, ((0, 128),))
    norm_gain = jnp.clip(1.0 + 0.18 * jax.random.normal(keys[1], (D,), jnp.float32), 0.1, 1.9)
    w_query = gaussian(keys[2], (D, INNER), D ** -0.5, 0.125, ((1, 2),))
    w_key = gaussian(keys[3], (D, INNER), D ** -0.5, 0.125, ((1, 2),))
    w_value = gaussian(keys[4], (D, INNER), D ** -0.5, 0.125, ((1, 2),))
    w_outgate = gaussian(keys[5], (D, INNER), D ** -0.5, 0.125, ((1, 2),))
    w_input_gate = gaussian(keys[6], (D, HEADS), D ** -0.5, 0.125)
    w_forget_gate = gaussian(keys[7], (D, HEADS), D ** -0.5, 0.125)
    forget_bias = jnp.clip(jax.random.uniform(keys[8], (HEADS,), jnp.float32, -1.0, 4.0), -1.0, 4.0)
    head_gain = jnp.clip(1.0 + 0.18 * jax.random.normal(keys[9], (INNER,), jnp.float32), 0.1, 1.9)
    w_output = gaussian(keys[10], (INNER, D), INNER ** -0.5, 0.21875, ((0, 2),))
    memory = gaussian(keys[11], (BATCH, HEADS, DH, DH), 0.3, 2.0, ((0, 128), (1, 2)), jnp.float32)
    normalizer = gaussian(keys[12], (BATCH, HEADS, DH), 0.3, 2.0, ((0, 128), (1, 2)), jnp.float32)
    stabilizer = jnp.clip(jax.random.uniform(keys[13], (BATCH, HEADS), jnp.float32, -2.0, 2.0) * block_levels(keys[13], (BATCH, HEADS), ((0, 128), (1, 2)), -0.4, 0.0), -2.0, 2.0)
    ffn_gain = jnp.clip(1.0 + 0.18 * jax.random.normal(keys[14], (D,), jnp.float32), 0.1, 1.9)
    route_ids_keys = jax.random.split(jax.random.fold_in(keys[15], 1), BATCH // B_DEV)
    route_ids_turns = jax.random.permutation(jax.random.fold_in(keys[15], 3), BATCH // B_DEV)
    route_ids = jax.vmap(lambda own, number: shared_out(jax.random.fold_in(keys[15], 2), own, number, B_DEV, EXPERTS, TOPK, CAP, 2))(route_ids_keys, route_ids_turns).reshape((BATCH, TOPK))
    route_probs = jnp.clip(jnp.exp(math.log(1.0) - 2.9957323 * jax.random.uniform(keys[16], (BATCH, TOPK), jnp.float32) ** block_levels(keys[16], (BATCH, TOPK), ((0, 128),), -0.2, 0.2)), 0.05, 1.0)
    expert_gate = gaussian(keys[17], (EXPERTS, D, FFE), D ** -0.5, 0.125, ((0, 128), (2, 2)))
    expert_up = gaussian(keys[18], (EXPERTS, D, FFE), D ** -0.5, 0.125, ((0, 128), (2, 2)))
    expert_down = gaussian(keys[19], (EXPERTS, FFE, D), FFE ** -0.5, 0.1875, ((0, 128), (1, 2)))
    return {"tokens": tokens, "norm_gain": norm_gain, "w_query": w_query, "w_key": w_key, "w_value": w_value, "w_outgate": w_outgate, "w_input_gate": w_input_gate, "w_forget_gate": w_forget_gate, "forget_bias": forget_bias, "head_gain": head_gain, "w_output": w_output, "memory": memory, "normalizer": normalizer, "stabilizer": stabilizer, "ffn_gain": ffn_gain, "route_ids": route_ids, "route_probs": route_probs, "expert_gate": expert_gate, "expert_up": expert_up, "expert_down": expert_down}


EPS = 1e-06

def rms_scaled(values, scales):
    floats = values.astype(jnp.float32)
    return floats * lax.rsqrt(lax.optimization_barrier(jnp.mean(floats * floats, axis=-1, keepdims=True)) + EPS) * scales.astype(jnp.float32)

def expert_apply(inputs):
    expert_rows, gate_w, up_w, down_w = inputs
    gate_val = jnp.dot(expert_rows, gate_w, preferred_element_type=jnp.float32)
    up_val = jnp.dot(expert_rows, up_w, preferred_element_type=jnp.float32)
    hidden = (jax.nn.silu(gate_val) * up_val).astype(jnp.bfloat16)
    half_width = FFE // N_TP
    summed = jnp.zeros((expert_rows.shape[0], D), jnp.float32)
    for tp_part in range(N_TP):
        partial_value = jnp.dot(hidden[:, tp_part * half_width:(tp_part + 1) * half_width], down_w[tp_part * half_width:(tp_part + 1) * half_width], preferred_element_type=jnp.float32).astype(jnp.bfloat16)
        summed = summed + lax.optimization_barrier(partial_value).astype(jnp.float32)
    return summed.astype(jnp.bfloat16)

def reference(tokens, norm_gain, w_query, w_key, w_value, w_outgate, w_input_gate, w_forget_gate, forget_bias, head_gain, w_output, memory, normalizer, stabilizer, ffn_gain, route_ids, route_probs, expert_gate, expert_up, expert_down):
    highest = lax.Precision.HIGHEST
    batch_rows = tokens.shape[0]
    normed = rms_scaled(tokens, norm_gain).astype(jnp.bfloat16)
    query = jnp.dot(normed, w_query, preferred_element_type=jnp.float32).reshape(batch_rows, HEADS, DH)
    key_vec = (jnp.dot(normed, w_key, preferred_element_type=jnp.float32) * DH ** (-0.5)).reshape(batch_rows, HEADS, DH)
    value_vec = jnp.dot(normed, w_value, preferred_element_type=jnp.float32).reshape(batch_rows, HEADS, DH)
    outgate = jnp.dot(normed, w_outgate, preferred_element_type=jnp.float32)
    input_pre = jnp.dot(normed, w_input_gate, preferred_element_type=jnp.float32)
    log_forget = jax.nn.log_sigmoid(jnp.dot(normed, w_forget_gate, preferred_element_type=jnp.float32) + forget_bias)
    new_stab = jnp.maximum(log_forget + stabilizer, input_pre)
    keep_gate = jnp.exp(log_forget + stabilizer - new_stab)
    write_gate = jnp.exp(input_pre - new_stab)
    new_memory = keep_gate[:, :, None, None] * memory + write_gate[:, :, None, None] * key_vec[:, :, :, None] * value_vec[:, :, None, :]
    new_normalizer = keep_gate[:, :, None] * normalizer + write_gate[:, :, None] * key_vec
    numerator = jnp.einsum('bhd,bhde->bhe', query, new_memory, precision=highest)
    denominator = lax.optimization_barrier(jnp.sum(query * new_normalizer, axis=-1))
    readout = numerator / jnp.maximum(jnp.abs(denominator), jnp.exp(-new_stab))[:, :, None]
    normed_read = readout * lax.rsqrt(lax.optimization_barrier(jnp.mean(readout * readout, axis=-1, keepdims=True)) + EPS) * head_gain.reshape(HEADS, DH)
    gated = (normed_read.reshape(batch_rows, HEADS * DH) * jax.nn.sigmoid(outgate)).astype(jnp.bfloat16)
    local_width = HEADS * DH // N_TP
    mix_sum = jnp.zeros((batch_rows, D), jnp.float32)
    for tp_part in range(N_TP):
        partial_value = jnp.dot(gated[:, tp_part * local_width:(tp_part + 1) * local_width], w_output[tp_part * local_width:(tp_part + 1) * local_width], preferred_element_type=jnp.float32).astype(jnp.bfloat16)
        mix_sum = mix_sum + lax.optimization_barrier(partial_value).astype(jnp.float32)
    mixed = mix_sum.astype(jnp.bfloat16)
    resid = (tokens.astype(jnp.float32) + mixed.astype(jnp.float32)).astype(jnp.bfloat16)
    ffn_in = rms_scaled(resid, ffn_gain).astype(jnp.bfloat16)
    weights = route_probs / lax.optimization_barrier(jnp.sum(route_probs, axis=-1, keepdims=True))
    flat_expert = route_ids.reshape(-1).astype(jnp.int32)
    onehot = (flat_expert[:, None] == jnp.arange(EXPERTS, dtype=jnp.int32)[None, :]).astype(jnp.int32)
    per_block = onehot.reshape(N_EP, B_DEV * TOPK, EXPERTS)
    earlier = jnp.cumsum(per_block, axis=1) - per_block
    slot_rank = lax.optimization_barrier(jnp.sum(earlier * per_block, axis=-1)).reshape(-1)
    route_index = jnp.arange(batch_rows * TOPK, dtype=jnp.int32)
    source = route_index // (B_DEV * TOPK)
    slot_index = (source * CAP + slot_rank).astype(jnp.int32)
    token_of = route_index // TOPK
    buffers = jnp.zeros((EXPERTS, N_EP * CAP, D), jnp.bfloat16).at[flat_expert, slot_index].set(ffn_in[token_of])
    results = lax.map(expert_apply, (buffers, expert_gate, expert_up, expert_down))
    picked = results[flat_expert, slot_index].astype(jnp.float32).reshape(batch_rows, TOPK, D)
    combined = lax.optimization_barrier(jnp.sum(picked * weights[:, :, None], axis=1))
    next_tokens = (resid.astype(jnp.float32) + combined).astype(jnp.bfloat16)
    return (next_tokens, new_memory, new_normalizer, new_stab)
```

```python
import functools

import jax
import jax.numpy as jnp
from jax import lax
from jax.experimental import pallas as pl
from jax.experimental.pallas import tpu as pltpu
from jax.sharding import PartitionSpec as P

EPS = 1e-06
PLANE = 16
BF16 = jnp.bfloat16
F32 = jnp.float32


def rms_scaled(values, scales):
    floats = values.astype(F32)
    return floats * lax.rsqrt(jnp.mean(floats * floats, axis=-1, keepdims=True) + EPS) * scales


def moe_kernel(
    nz,
    ng,
    part_ref,
    tok_ref,
    gain_ref,
    meta_ref,
    wg_hbm,
    wu_hbm,
    wd_hbm,
    out_ref,
    wg,
    wu,
    wd,
    pbuf,
    meta,
    zrows,
    snd,
    rcv,
    osnd,
    back,
    zsnd,
    zrcv,
    hbuf,
    w_sem,
    p_sem,
    m_sem,
    z_sem,
    d_sem,
    b_sem,
    r_sem,
    f_sem,
):
    ep = lax.axis_index("ep")
    tp = lax.axis_index("tp")
    z = ep // ng
    g = ep % ng
    me = g * 2 + tp
    other = 1 - tp
    np_ = 2 * ng
    rows = tok_ref.shape[0]
    half = tok_ref.shape[1] // 2
    slots = 2 * nz

    weights = [
        pltpu.make_async_copy(src, dst, w_sem.at[i])
        for i, (src, dst) in enumerate(((wg_hbm, wg), (wu_hbm, wu), (wd_hbm, wd)))
    ]
    for copy in weights:
        copy.start()

    barrier = pltpu.get_barrier_semaphore()

    @pl.loop(1, nz)
    def _(d):
        pl.semaphore_signal(barrier, inc=1, device_id=(lax.rem(z + d, nz) * ng + g, tp))

    @pl.loop(1, np_)
    def _(d):
        q = lax.rem(me + d, np_)
        pl.semaphore_signal(barrier, inc=1, device_id=(z * ng + q // 2, q % 2))

    pl.semaphore_wait(barrier, nz - 1 + np_ - 1)

    def remote(src, dst, sems, at_src, at_dst, to_ep, to_tp):
        return pltpu.make_async_remote_copy(
            src_ref=src,
            dst_ref=dst,
            send_sem=sems.at[0, at_src],
            recv_sem=sems.at[1, at_dst],
            device_id=(to_ep, to_tp),
        )

    swap = remote(part_ref, pbuf, p_sem, 0, 0, ep, other)
    swap.start()

    def meta_copy(d, at):
        to = lax.rem(z + d, nz)
        return remote(meta_ref, meta.at[at], m_sem, d, at, to * ng + g, tp)

    @pl.loop(1, nz)
    def _(d):
        meta_copy(d, z).start()

    meta[z] = meta_ref[...]

    @pl.loop(1, nz)
    def _(d):
        meta_copy(d, lax.rem(z + d, nz)).wait_recv()

    base = (z * (ng * slots) + 1).astype(F32)
    code_t = meta[0][rows:, :]
    for s in range(1, nz):
        code_t = code_t + meta[s][rows:, :]
    code_t = (code_t - base).astype(jnp.int32)
    lanes = nz * rows
    slot_at = lax.broadcasted_iota(jnp.int32, (ng * slots, lanes), 0)
    pick = jnp.zeros((ng * slots, lanes), F32)
    for k in range(4):
        pick = pick + jnp.where(slot_at == code_t[k : k + 1, :lanes], 1.0, 0.0)
    pick = pick.astype(BF16)
    by_row = meta[:, :rows, :].reshape(lanes, meta.shape[2])
    code_r = (by_row[:, 0:4] - base).astype(jnp.int32)
    slot_at = lax.broadcasted_iota(jnp.int32, (lanes, ng * slots), 1)
    mix = jnp.zeros((lanes, ng * slots), F32)
    for k in range(4):
        mix = mix + jnp.where(slot_at == code_r[:, k : k + 1], by_row[:, 4 + k : 5 + k], 0.0)
    mix_hi = mix.astype(BF16)
    mix_lo = (mix - mix_hi.astype(F32)).astype(BF16)

    swap.wait_recv()
    mixed = (part_ref[...].astype(F32) + pbuf[...].astype(F32)).astype(BF16)
    resid = (tok_ref[...].astype(F32) + mixed.astype(F32)).astype(BF16)
    ffn_in = rms_scaled(resid, gain_ref[...]).astype(BF16)

    def my_half(values):
        return jnp.where(tp == 0, values[:, :half], values[:, half:])

    zrows[z] = my_half(ffn_in)

    def z_copy(d, at):
        to = lax.rem(z + d, nz)
        return remote(zrows.at[z], zrows.at[at], z_sem, d, at, to * ng + g, tp)

    @pl.loop(1, nz)
    def _(d):
        z_copy(d, z).start()

    @pl.loop(1, nz)
    def _(d):
        z_copy(d, lax.rem(z + d, nz)).wait_recv()

    gathered = zrows[...].reshape(lanes, half)
    snd[...] = (
        jnp.dot(pick, gathered, preferred_element_type=F32).astype(BF16).reshape(ng, slots, half)
    )

    def d_copy(d, at):
        q = lax.rem(me + d, np_)
        to_g, to_tp = q // 2, q % 2
        return remote(
            snd.at[to_g], rcv.at[at % 2, at // 2], d_sem, d, at, z * ng + to_g, to_tp
        )

    @pl.loop(1, np_)
    def _(d):
        d_copy(d, me).start()

    rcv[tp, g] = snd[g]
    for copy in weights:
        copy.wait()

    @pl.loop(1, np_)
    def _(d):
        d_copy(d, lax.rem(me + d, np_)).wait_recv()

    left = rcv[0].reshape(ng * slots, half)
    right = rcv[1].reshape(ng * slots, half)

    def both(w):
        return jnp.dot(left, w[:half, :], preferred_element_type=F32) + jnp.dot(
            right, w[half:, :], preferred_element_type=F32
        )

    gate_val = both(wg)
    hidden = (gate_val * jax.nn.sigmoid(gate_val) * both(wu)).astype(BF16)
    for h in range(2):
        osnd[h] = (
            jnp.dot(hidden, wd[:, h * half : (h + 1) * half], preferred_element_type=F32)
            .astype(BF16)
            .reshape(ng, slots, half)
        )

    def b_copy(d, at):
        q = lax.rem(me + d, np_)
        to_g, to_tp = q // 2, q % 2
        return remote(
            osnd.at[to_tp, to_g], back.at[at % 2, at // 2], b_sem, d, at, z * ng + to_g, to_tp
        )

    @pl.loop(1, np_)
    def _(d):
        b_copy(d, me).start()

    back[tp, g] = osnd[tp, g]

    @pl.loop(1, np_)
    def _(d):
        b_copy(d, lax.rem(me + d, np_)).wait_recv()

    served = (back[0].astype(F32) + back[1].astype(F32)).astype(BF16).reshape(ng * slots, half)
    sums = jnp.dot(mix_hi, served, preferred_element_type=F32) + jnp.dot(
        mix_lo, served, preferred_element_type=F32
    )
    zsnd[...] = sums.astype(BF16).reshape(nz, rows, half)

    def r_copy(d, at):
        to = lax.rem(z + d, nz)
        return remote(zsnd.at[to], zrcv.at[at], r_sem, d, at, to * ng + g, tp)

    @pl.loop(1, nz)
    def _(d):
        r_copy(d, z).start()

    zrcv[z] = zsnd[z]

    @pl.loop(1, nz)
    def _(d):
        r_copy(d, lax.rem(z + d, nz)).wait_recv()

    total = my_half(resid).astype(F32)
    for s in range(nz):
        total = total + zrcv[s].astype(F32)
    mine = total.astype(BF16)
    hbuf[0] = mine
    last = remote(hbuf.at[0], hbuf.at[1], f_sem, 0, 0, ep, other)
    last.start()
    last.wait_recv()
    theirs = hbuf[1]
    real = out_ref.shape[0]
    out_ref[:, :half] = jnp.where(tp == 0, mine, theirs)[:real]
    out_ref[:, half:] = jnp.where(tp == 0, theirs, mine)[:real]

    swap.wait_send()
    last.wait_send()

    @pl.loop(1, nz)
    def _(d):
        meta_copy(d, z).wait_send()
        z_copy(d, z).wait_send()
        r_copy(d, z).wait_send()

    @pl.loop(1, np_)
    def _(d):
        d_copy(d, me).wait_send()
        b_copy(d, me).wait_send()


def moe(nz, ng, part, tok, gain, meta, wg, wu, wd, real):
    rows, width = tok.shape
    half = width // 2
    slots = 2 * nz
    vmem = pl.BlockSpec(memory_space=pltpu.VMEM)
    hbm = pl.BlockSpec(memory_space=pl.ANY)

    def sems(n):
        return pltpu.SemaphoreType.DMA((2, n))

    return pl.pallas_call(
        functools.partial(moe_kernel, nz, ng),
        out_shape=jax.ShapeDtypeStruct((real, width), BF16),
        in_specs=[vmem] * 4 + [hbm] * 3,
        out_specs=vmem,
        scratch_shapes=[
            pltpu.VMEM(wg.shape, BF16),
            pltpu.VMEM(wu.shape, BF16),
            pltpu.VMEM(wd.shape, BF16),
            pltpu.VMEM((rows, width), BF16),
            pltpu.VMEM((nz, *meta.shape), F32),
            pltpu.VMEM((nz, rows, half), BF16),
            pltpu.VMEM((ng, slots, half), BF16),
            pltpu.VMEM((2, ng, slots, half), BF16),
            pltpu.VMEM((2, ng, slots, half), BF16),
            pltpu.VMEM((2, ng, slots, half), BF16),
            pltpu.VMEM((nz, rows, half), BF16),
            pltpu.VMEM((nz, rows, half), BF16),
            pltpu.VMEM((2, rows, half), BF16),
            pltpu.SemaphoreType.DMA((3,)),
            sems(1),
            sems(nz),
            sems(nz),
            sems(2 * ng),
            sems(2 * ng),
            sems(nz),
            sems(1),
        ],
        compiler_params=pltpu.CompilerParams(
            collective_id=0, has_side_effects=True, vmem_limit_bytes=48 << 20
        ),
        name="experts",
    )(part, tok, gain, meta, wg, wu, wd)


def route_meta(z, nz, rows, route_ids, route_probs):
    count, top = route_ids.shape
    same = route_ids[:, :, None, None] == route_ids[None, None, :, :]
    before = jnp.arange(count)[None, :] < jnp.arange(count)[:, None]
    rank = jnp.sum((same & before[:, None, :, None]).astype(jnp.int32), axis=(2, 3))
    code = (route_ids * (2 * nz) + 2 * z + rank + 1).astype(F32)
    weights = route_probs / jnp.sum(route_probs, axis=-1, keepdims=True)
    by_row = jnp.pad(jnp.concatenate([code, weights], axis=1), ((0, rows - count), (0, 128 - 2 * top)))
    spread = (jnp.arange(nz) == z).astype(F32)[None, :, None] * jnp.pad(
        code.T, ((0, 8 - top), (0, rows - count))
    )[:, None, :]
    by_lane = jnp.pad(spread.reshape(8, nz * rows), ((0, 0), (0, 128 - nz * rows)))
    return jnp.concatenate([by_row, by_lane], axis=0)


def local(
    tokens,
    norm_gain,
    w_query,
    w_key,
    w_value,
    w_outgate,
    w_input_gate,
    w_forget_gate,
    forget_bias,
    head_gain,
    w_output,
    memory,
    normalizer,
    stabilizer,
    ffn_gain,
    route_ids,
    route_probs,
    expert_gate,
    expert_up,
    expert_down,
):
    tp_rank = lax.axis_index("tp")
    ep_count = lax.axis_size("ep")
    ng = min(PLANE, ep_count // 2)
    nz = ep_count // ng
    dev_rows, width = tokens.shape
    dev_heads = memory.shape[1]
    head_dim = memory.shape[2]
    local_width = dev_heads * head_dim
    normed = rms_scaled(tokens, norm_gain).astype(jnp.bfloat16)
    query = jnp.dot(normed, w_query, preferred_element_type=jnp.float32)
    key_raw = jnp.dot(normed, w_key, preferred_element_type=jnp.float32)
    value_raw = jnp.dot(normed, w_value, preferred_element_type=jnp.float32)
    outgate = jnp.dot(normed, w_outgate, preferred_element_type=jnp.float32)
    head_start = tp_rank * dev_heads
    input_cols = lax.dynamic_slice_in_dim(w_input_gate, head_start, dev_heads, 1)
    forget_cols = lax.dynamic_slice_in_dim(w_forget_gate, head_start, dev_heads, 1)
    bias_part = lax.dynamic_slice_in_dim(forget_bias, head_start, dev_heads, 0)
    gain_part = lax.dynamic_slice_in_dim(head_gain, tp_rank * local_width, local_width, 0)
    query = query.reshape(dev_rows, dev_heads, head_dim)
    key_vec = (key_raw * head_dim ** (-0.5)).reshape(dev_rows, dev_heads, head_dim)
    value_vec = value_raw.reshape(dev_rows, dev_heads, head_dim)
    input_pre = jnp.dot(normed, input_cols, preferred_element_type=jnp.float32)
    log_forget = jax.nn.log_sigmoid(
        jnp.dot(normed, forget_cols, preferred_element_type=jnp.float32) + bias_part
    )
    new_stab = jnp.maximum(log_forget + stabilizer, input_pre)
    keep_gate = jnp.exp(log_forget + stabilizer - new_stab)
    write_gate = jnp.exp(input_pre - new_stab)
    new_memory = (
        keep_gate[:, :, None, None] * memory
        + write_gate[:, :, None, None] * key_vec[:, :, :, None] * value_vec[:, :, None, :]
    )
    new_normalizer = keep_gate[:, :, None] * normalizer + write_gate[:, :, None] * key_vec
    numerator = jnp.einsum("bhd,bhde->bhe", query, new_memory)
    denominator = jnp.sum(query * new_normalizer, axis=-1)
    readout = numerator / jnp.maximum(jnp.abs(denominator), jnp.exp(-new_stab))[:, :, None]
    normed_read = (
        readout
        * lax.rsqrt(jnp.mean(readout * readout, axis=-1, keepdims=True) + EPS)
        * gain_part.reshape(dev_heads, head_dim)
    )
    gated = (normed_read.reshape(dev_rows, local_width) * jax.nn.sigmoid(outgate)).astype(
        jnp.bfloat16
    )
    rows = -(-dev_rows // 16) * 16
    pad = ((0, rows - dev_rows), (0, 0))
    partial_value = jnp.dot(
        jnp.pad(gated, pad), w_output, preferred_element_type=jnp.float32
    ).astype(jnp.bfloat16)
    meta = route_meta(lax.axis_index("ep") // ng, nz, rows, route_ids, route_probs)
    next_tokens = moe(
        nz,
        ng,
        partial_value,
        jnp.pad(tokens, pad),
        ffn_gain.reshape(1, width),
        meta,
        expert_gate[0],
        expert_up[0],
        expert_down[0],
        dev_rows,
    )
    return (next_tokens, new_memory, new_normalizer, new_stab)


def solution(mesh):
    return jax.shard_map(
        local,
        mesh=mesh,
        in_specs=(
            P("ep", None),
            P(),
            P(None, "tp"),
            P(None, "tp"),
            P(None, "tp"),
            P(None, "tp"),
            P(),
            P(),
            P(),
            P(),
            P("tp", None),
            P("ep", "tp", None, None),
            P("ep", "tp", None),
            P("ep", "tp"),
            P(),
            P("ep", None),
            P("ep", None),
            P("ep", None, "tp"),
            P("ep", None, "tp"),
            P("ep", "tp", None),
        ),
        out_specs=(P("ep", None), P("ep", "tp", None, None), P("ep", "tp", None), P("ep", "tp")),
        check_vma=False,
    )
```

```python
import functools

import jax
import jax.numpy as jnp
from jax import lax
from jax.experimental import pallas as pl
from jax.experimental.pallas import tpu as pltpu
from jax.sharding import PartitionSpec as P

EPS = 1e-06
PLANE = 16
FULL_VMEM = 67043328
BF16 = jnp.bfloat16
F32 = jnp.float32


def rms_scaled(values, scales):
    floats = values.astype(F32)
    return floats * lax.rsqrt(jnp.mean(floats * floats, axis=-1, keepdims=True) + EPS) * scales


def place_of(d, nz):
    if d == 0:
        return 0
    return 2 * d - 1 if d <= nz // 2 else 2 * (nz - d)


def moe_kernel(
    nz,
    ng,
    gated_ref,
    meta_ref,
    wout_hbm,
    tok_hbm,
    gain_hbm,
    wg_hbm,
    wu_hbm,
    wd_hbm,
    out_ref,
    wout,
    tok_ref,
    gain_ref,
    wg,
    wu,
    wd,
    pbuf,
    meta,
    zrows,
    snd,
    rcv,
    osnd,
    back,
    zsnd,
    zrcv,
    hbuf,
    w_sem,
    p_sem,
    m_sem,
    z_sem,
    d_sem,
    b_sem,
    r_sem,
    f_sem,
):
    ep = lax.axis_index("ep")
    tp = lax.axis_index("tp")
    z = ep // ng
    g = ep % ng
    me = g * 2 + tp
    other = 1 - tp
    np_ = 2 * ng
    count, width = tok_ref.shape
    rows, half = zrows.shape[1:]
    per = nz // 2
    slots = 2 * per

    copies = [
        pltpu.make_async_copy(src, dst, w_sem.at[i])
        for i, (src, dst) in enumerate(
            (
                (wout_hbm, wout),
                (tok_hbm, tok_ref),
                (gain_hbm, gain_ref),
                (wg_hbm, wg),
                (wu_hbm, wu),
                (wd_hbm, wd),
            )
        )
    ]
    weights = copies[3:]
    for copy in copies:
        copy.start()

    barrier = pltpu.get_barrier_semaphore()

    @pl.loop(1, nz)
    def _(d):
        pl.semaphore_signal(barrier, inc=1, device_id=(lax.rem(z + d, nz) * ng + g, tp))

    @pl.loop(1, np_)
    def _(d):
        q = lax.rem(me + d, np_)
        pl.semaphore_signal(barrier, inc=1, device_id=(z * ng + q // 2, q % 2))

    copies[0].wait()
    pbuf[0] = jnp.dot(gated_ref[...], wout[...], preferred_element_type=F32).astype(BF16)
    meta[0] = meta_ref[...]
    pl.semaphore_wait(barrier, nz - 1 + np_ - 1)

    def remote(src, dst, sems, at_src, at_dst, to_ep, to_tp):
        return pltpu.make_async_remote_copy(
            src_ref=src,
            dst_ref=dst,
            send_sem=sems.at[0, at_src],
            recv_sem=sems.at[1, at_dst],
            device_id=(to_ep, to_tp),
        )

    def along_z(sems, source, target):
        sent, arriving = {}, {}
        for d in range(1, nz):
            there, here = place_of(nz - d, nz), place_of(d, nz)
            to = lax.rem(z + d, nz) * ng + g
            sent[here] = remote(source(here), target(there), sems, here, there, to, tp)
            arriving[here] = remote(source(here), target(here), sems, here, here, to, tp)
        return sent, arriving

    swap = remote(pbuf.at[0], pbuf.at[1], p_sem, 0, 0, ep, other)
    swap.start()
    meta_out, meta_in = along_z(m_sem, lambda o: meta.at[0], lambda o: meta.at[o])
    for o in range(1, nz):
        meta_out[o].start()

    copies[1].wait()
    copies[2].wait()
    swap.wait_recv()
    mixed = (pbuf[0].astype(F32) + pbuf[1].astype(F32)).astype(BF16)
    resid = (tok_ref[...].astype(F32) + mixed.astype(F32)).astype(BF16)
    ffn_in = rms_scaled(resid, gain_ref[...]).astype(BF16)

    def my_half(values):
        return jnp.where(tp == 0, values[:, :half], values[:, half:])

    if rows > count:
        zrows[0] = jnp.zeros((rows, half), BF16)
    zrows[0, :count, :] = my_half(ffn_in)
    z_out, z_in = along_z(z_sem, lambda o: zrows.at[0], lambda o: zrows.at[o])
    for o in range(1, nz):
        z_out[o].start()

    for o in range(1, nz):
        meta_in[o].wait_recv()

    first = (z * ng + 1).astype(F32)
    lanes = per * rows
    picks, mixes = [], []
    for c in range(2):
        whole = [
            meta[c * per + i, rows:, :] if i == 0 else pltpu.roll(meta[c * per + i, rows:, :], i * rows, 1)
            for i in range(per)
        ]
        by_lane = whole[0]
        for part in whole[1:]:
            by_lane = by_lane + part
        source = lax.broadcasted_iota(jnp.int32, (4, lanes), 1) // rows
        slot_t = (
            (by_lane[0:4, :lanes] - first) * slots + by_lane[4:8, :lanes]
        ).astype(jnp.int32) + 2 * source
        slot_at = lax.broadcasted_iota(jnp.int32, (ng * slots, lanes), 0)
        pick = jnp.zeros((ng * slots, lanes), F32)
        for k in range(4):
            pick = pick + jnp.where(slot_at == slot_t[k : k + 1, :], 1.0, 0.0)
        picks.append(pick.astype(BF16))
        by_row = meta[c * per : (c + 1) * per, :rows, :].reshape(lanes, meta.shape[2])
        source = lax.broadcasted_iota(jnp.int32, (lanes, 4), 0) // rows
        slot_r = ((by_row[:, 0:4] - first) * slots + by_row[:, 8:12]).astype(jnp.int32) + 2 * source
        slot_at = lax.broadcasted_iota(jnp.int32, (lanes, ng * slots), 1)
        mix = jnp.zeros((lanes, ng * slots), F32)
        for k in range(4):
            mix = mix + jnp.where(slot_at == slot_r[:, k : k + 1], by_row[:, 4 + k : 5 + k], 0.0)
        mix_hi = mix.astype(BF16)
        mixes.append((mix_hi, (mix - mix_hi.astype(F32)).astype(BF16)))

    def d_copy(c, d, at):
        q = lax.rem(me + d, np_)
        to_g, to_tp = q // 2, q % 2
        return remote(
            snd.at[c, to_g],
            rcv.at[c, at % 2, at // 2],
            d_sem.at[c],
            d,
            at,
            z * ng + to_g,
            to_tp,
        )

    for c in range(2):
        for o in range(max(1, c * per), (c + 1) * per):
            z_in[o].wait_recv()
        gathered = zrows[c * per : (c + 1) * per].reshape(lanes, half)
        snd[c] = (
            jnp.dot(picks[c], gathered, preferred_element_type=F32)
            .astype(BF16)
            .reshape(ng, slots, half)
        )

        @pl.loop(1, np_)
        def _(d):
            d_copy(c, d, me).start()

        rcv[c, tp, g] = snd[c, g]

    for copy in weights:
        copy.wait()

    def b_copy(c, d, at):
        q = lax.rem(me + d, np_)
        to_g, to_tp = q // 2, q % 2
        return remote(
            osnd.at[c, to_tp, to_g],
            back.at[c, at % 2, at // 2],
            b_sem.at[c],
            d,
            at,
            z * ng + to_g,
            to_tp,
        )

    for c in range(2):

        @pl.loop(1, np_)
        def _(d):
            d_copy(c, d, lax.rem(me + d, np_)).wait_recv()

        left = rcv[c, 0].reshape(ng * slots, half)
        right = rcv[c, 1].reshape(ng * slots, half)

        def both(w):
            return jnp.dot(left, w[:half, :], preferred_element_type=F32) + jnp.dot(
                right, w[half:, :], preferred_element_type=F32
            )

        gate_val = both(wg)
        hidden = (gate_val * jax.nn.sigmoid(gate_val) * both(wu)).astype(BF16)
        for h in range(2):
            osnd[c, h] = (
                jnp.dot(hidden, wd[:, h * half : (h + 1) * half], preferred_element_type=F32)
                .astype(BF16)
                .reshape(ng, slots, half)
            )

        @pl.loop(1, np_)
        def _(d):
            b_copy(c, d, me).start()

        back[c, tp, g] = osnd[c, tp, g]

    r_out, r_in = along_z(r_sem, lambda o: zsnd.at[o], lambda o: zrcv.at[o])
    for c in range(2):

        @pl.loop(1, np_)
        def _(d):
            b_copy(c, d, lax.rem(me + d, np_)).wait_recv()

        served = (
            (back[c, 0].astype(F32) + back[c, 1].astype(F32)).astype(BF16).reshape(ng * slots, half)
        )
        mix_hi, mix_lo = mixes[c]
        sums = jnp.dot(mix_hi, served, preferred_element_type=F32) + jnp.dot(
            mix_lo, served, preferred_element_type=F32
        )
        zsnd[c * per : (c + 1) * per] = sums.astype(BF16).reshape(per, rows, half)
        for o in range(max(1, c * per), (c + 1) * per):
            r_out[o].start()

    total = my_half(resid).astype(F32) + zsnd[0, :count, :].astype(F32)
    for o in range(1, nz):
        r_in[o].wait_recv()
        total = total + zrcv[o, :count, :].astype(F32)
    mine = total.astype(BF16)
    hbuf[0] = mine
    last = remote(hbuf.at[0], hbuf.at[1], f_sem, 0, 0, ep, other)
    last.start()
    last.wait_recv()
    theirs = hbuf[1]
    out_ref[:, :half] = jnp.where(tp == 0, mine, theirs)
    out_ref[:, half:] = jnp.where(tp == 0, theirs, mine)

    swap.wait_send()
    last.wait_send()
    for o in range(1, nz):
        meta_out[o].wait_send()
        z_out[o].wait_send()
        r_out[o].wait_send()
    for c in range(2):

        @pl.loop(1, np_)
        def _(d):
            d_copy(c, d, me).wait_send()
            b_copy(c, d, me).wait_send()


def moe(nz, ng, gated, meta, wout, tok, gain, wg, wu, wd):
    count, width = tok.shape
    rows = meta.shape[0] - 8
    half = width // 2
    vmem = pl.BlockSpec(memory_space=pltpu.VMEM)
    hbm = pl.BlockSpec(memory_space=pltpu.HBM)

    def sems(*n):
        return pltpu.SemaphoreType.DMA(n)

    return pl.pallas_call(
        functools.partial(moe_kernel, nz, ng),
        out_shape=jax.ShapeDtypeStruct((count, width), BF16),
        in_specs=[vmem] * 2 + [hbm] * 6,
        out_specs=vmem,
        scratch_shapes=[pltpu.VMEM(a.shape, a.dtype) for a in (wout, tok, gain, wg, wu, wd)]
        + [
            pltpu.VMEM((2, count, width), BF16),
            pltpu.VMEM((nz, *meta.shape), F32),
            pltpu.VMEM((nz, rows, half), BF16),
            pltpu.VMEM((2, ng, nz, half), BF16),
            pltpu.VMEM((2, 2, ng, nz, half), BF16),
            pltpu.VMEM((2, 2, ng, nz, half), BF16),
            pltpu.VMEM((2, 2, ng, nz, half), BF16),
            pltpu.VMEM((nz, rows, half), BF16),
            pltpu.VMEM((nz, rows, half), BF16),
            pltpu.VMEM((2, count, half), BF16),
            sems(6),
            sems(2, 1),
            sems(2, nz),
            sems(2, nz),
            sems(2, 2, 2 * ng),
            sems(2, 2, 2 * ng),
            sems(2, nz),
            sems(2, 1),
        ],
        compiler_params=pltpu.CompilerParams(
            collective_id=0, has_side_effects=True, vmem_limit_bytes=FULL_VMEM
        ),
        name="experts",
    )(gated, meta, wout, tok, gain, wg, wu, wd)


def cell_kernel(
    tok_hbm,
    ngain_hbm,
    wi_hbm,
    wf_hbm,
    bias_hbm,
    hgain_hbm,
    norm_hbm,
    stab_hbm,
    ids_hbm,
    probs_hbm,
    wq_hbm,
    wk_hbm,
    wv_hbm,
    wo_hbm,
    mem_hbm,
    gated_ref,
    meta_ref,
    nnorm_ref,
    nstab_ref,
    nmem_hbm,
    tok_ref,
    ngain_ref,
    wi_ref,
    wf_ref,
    bias_ref,
    hgain_ref,
    norm_ref,
    stab_ref,
    ids_ref,
    probs_ref,
    wq,
    wk,
    wv,
    wo,
    mem,
    num,
    s_sem,
    w_sem,
    in_sem,
    out_sem,
):
    tp = lax.axis_index("tp")
    count, width = tok_ref.shape
    heads, dim = norm_ref.shape[1:]
    small = [
        pltpu.make_async_copy(src, dst, s_sem.at[i])
        for i, (src, dst) in enumerate(
            (
                (ids_hbm, ids_ref),
                (probs_hbm, probs_ref),
                (tok_hbm, tok_ref),
                (ngain_hbm, ngain_ref),
                (wi_hbm, wi_ref),
                (wf_hbm, wf_ref),
                (bias_hbm, bias_ref),
                (stab_hbm, stab_ref),
                (norm_hbm, norm_ref),
                (hgain_hbm, hgain_ref),
            )
        )
    ]
    loads = [
        pltpu.make_async_copy(src, dst, w_sem.at[i])
        for i, (src, dst) in enumerate(
            ((wk_hbm, wk), (wv_hbm, wv), (wq_hbm, wq), (wo_hbm, wo))
        )
    ]
    reads = [pltpu.make_async_copy(mem_hbm.at[b], mem.at[b], in_sem.at[b]) for b in range(count)]
    writes = [pltpu.make_async_copy(mem.at[b], nmem_hbm.at[b], out_sem.at[b]) for b in range(count)]
    for copy in small + loads + reads:
        copy.start()

    for copy in small:
        copy.wait()
    ids = ids_ref[...].astype(F32).T.astype(jnp.int32)
    probs = probs_ref[...].T
    weights = probs / jnp.sum(probs, axis=-1, keepdims=True)
    lane = lax.broadcasted_iota(jnp.int32, (count, 128), 1)
    row = lax.broadcasted_iota(jnp.int32, (count, 128), 0)
    top = ids.shape[1]
    named = [lane == ids[:, k : k + 1] for k in range(top)]
    onehot = jnp.zeros((count, 128), F32)
    for k in range(top):
        onehot = onehot + jnp.where(named[k], 1.0, 0.0)
    rows16 = meta_ref.shape[0] - 8
    lower = lax.broadcasted_iota(jnp.int32, (count, count), 0) > lax.broadcasted_iota(
        jnp.int32, (count, count), 1
    )
    earlier = jnp.dot(
        jnp.where(lower, 1.0, 0.0).astype(BF16), onehot.astype(BF16), preferred_element_type=F32
    )
    by_row = jnp.zeros((count, 128), F32)
    meta_ref[...] = jnp.zeros(meta_ref.shape, F32)
    for k in range(top):
        rank = jnp.sum(jnp.where(named[k], earlier, 0.0), axis=1, keepdims=True)
        code = ids[:, k : k + 1].astype(F32) + 1.0
        for at, what in ((k, code), (4 + k, weights[:, k : k + 1]), (8 + k, rank)):
            by_row = jnp.where(lane == at, what, by_row)
        for at, what in ((k, code), (4 + k, rank)):
            meta_ref[rows16 + at : rows16 + at + 1, :] = jnp.sum(
                jnp.where(lane == row, what, 0.0), axis=0, keepdims=True
            )
    meta_ref[:count, :] = by_row

    normed = rms_scaled(tok_ref[...], ngain_ref[...]).astype(BF16)
    across = (((1,), (1,)), ((), ()))
    pre_all = lax.dot_general(normed, wi_ref[...], across, preferred_element_type=F32)
    forget_all = jax.nn.log_sigmoid(
        lax.dot_general(normed, wf_ref[...], across, preferred_element_type=F32) + bias_ref[...]
    )

    def project(i, w):
        loads[i].wait()
        return jnp.dot(normed, w[...], preferred_element_type=F32)

    key = project(0, wk) * dim ** (-0.5)
    value = project(1, wv)
    query = project(2, wq)
    outgate = project(3, wo)
    query_t = query.T
    stab = stab_ref[...].T
    new_stabs = []
    keeps, values, keys_t, floors = [], [], [], []
    for h in range(heads):
        pre = jnp.where(tp == 0, pre_all[:, h : h + 1], pre_all[:, heads + h : heads + h + 1])
        forget = jnp.where(
            tp == 0, forget_all[:, h : h + 1], forget_all[:, heads + h : heads + h + 1]
        )
        carried = forget + stab[:, h : h + 1]
        new_stab = jnp.maximum(carried, pre)
        new_stabs.append(new_stab)
        keep = jnp.exp(carried - new_stab)
        at = slice(h * dim, (h + 1) * dim)
        written = jnp.exp(pre - new_stab) * key[:, at]
        new_norm = keep * norm_ref[:, h, :] + written
        nnorm_ref[:, h, :] = new_norm
        den = jnp.sum(query[:, at] * new_norm, axis=1, keepdims=True)
        floors.append(jnp.maximum(jnp.abs(den), jnp.exp(-new_stab)))
        keeps.append(jnp.broadcast_to(keep, (count, dim)))
        values.append(value[:, at])
        keys_t.append(written.T)
    heads_at = lax.broadcasted_iota(jnp.int32, (count, heads), 1)
    both_stabs = jnp.broadcast_to(new_stabs[0], (count, heads))
    for h in range(1, heads):
        both_stabs = jnp.where(heads_at == h, new_stabs[h], both_stabs)
    nstab_ref[...] = both_stabs.T
    for b in range(count):
        reads[b].wait()
        for h in range(heads):
            new = keeps[h][b : b + 1, :] * mem[b, h] + (
                keys_t[h][:, b : b + 1] * values[h][b : b + 1, :]
            )
            mem[b, h] = new
            num[h, b : b + 1, :] = jnp.sum(
                query_t[h * dim : (h + 1) * dim, b : b + 1] * new, axis=0, keepdims=True
            )
        writes[b].start()
    local_width = heads * dim
    parts = local_width // 128
    gains = jnp.concatenate(
        [
            jnp.where(tp == 0, hgain_ref[i : i + 1, :], hgain_ref[parts + i : parts + i + 1, :])
            for i in range(parts)
        ],
        axis=1,
    )
    for h in range(heads):
        at = slice(h * dim, (h + 1) * dim)
        readout = num[h] / floors[h]
        scaled = (
            readout
            * lax.rsqrt(jnp.mean(readout * readout, axis=-1, keepdims=True) + EPS)
            * gains[:, at]
        )
        gated_ref[:, at] = (scaled * jax.nn.sigmoid(outgate[:, at])).astype(BF16)
    for copy in writes:
        copy.wait()


def cell(small, weights, memory):
    count, width = small[0].shape
    rows16 = -(-count // 16) * 16
    norm_shape = small[6].shape
    vmem = pl.BlockSpec(memory_space=pltpu.VMEM)
    hbm = pl.BlockSpec(memory_space=pltpu.HBM)
    return pl.pallas_call(
        cell_kernel,
        out_shape=(
            jax.ShapeDtypeStruct((count, weights[0].shape[1]), BF16),
            jax.ShapeDtypeStruct((rows16 + 8, 128), F32),
            jax.ShapeDtypeStruct(norm_shape, F32),
            jax.ShapeDtypeStruct((norm_shape[1], count), F32),
            jax.ShapeDtypeStruct(memory.shape, F32),
        ),
        in_specs=[hbm] * (len(small) + len(weights) + 1),
        out_specs=(vmem, vmem, vmem, vmem, hbm),
        scratch_shapes=[pltpu.VMEM(a.shape, a.dtype) for a in (*small, *weights, memory)]
        + [
            pltpu.VMEM((norm_shape[1], count, norm_shape[2]), F32),
            pltpu.SemaphoreType.DMA((len(small),)),
            pltpu.SemaphoreType.DMA((len(weights),)),
            pltpu.SemaphoreType.DMA((count,)),
            pltpu.SemaphoreType.DMA((count,)),
        ],
        compiler_params=pltpu.CompilerParams(vmem_limit_bytes=FULL_VMEM),
        name="cell",
    )(*small, *weights, memory)


def local(
    tokens,
    norm_gain,
    w_query,
    w_key,
    w_value,
    w_outgate,
    w_input_gate,
    w_forget_gate,
    forget_bias,
    head_gain,
    w_output,
    memory,
    normalizer,
    stabilizer,
    ffn_gain,
    route_ids,
    route_probs,
    expert_gate,
    expert_up,
    expert_down,
):
    ep_count = lax.axis_size("ep")
    ng = min(PLANE, ep_count // 2)
    nz = ep_count // ng
    gated, meta, new_normalizer, new_stab, new_memory = cell(
        (
            tokens,
            norm_gain.reshape(1, -1),
            w_input_gate.T,
            w_forget_gate.T,
            forget_bias.reshape(1, -1),
            head_gain.reshape(-1, 128),
            normalizer,
            stabilizer.T,
            route_ids.T,
            route_probs.T,
        ),
        (w_query, w_key, w_value, w_outgate),
        memory,
    )
    next_tokens = moe(
        nz,
        ng,
        gated,
        meta,
        w_output,
        tokens,
        ffn_gain.reshape(1, -1),
        expert_gate[0],
        expert_up[0],
        expert_down[0],
    )
    return (next_tokens, new_memory, new_normalizer, new_stab.T)


def solution(mesh):
    return jax.shard_map(
        local,
        mesh=mesh,
        in_specs=(
            P("ep", None),
            P(),
            P(None, "tp"),
            P(None, "tp"),
            P(None, "tp"),
            P(None, "tp"),
            P(),
            P(),
            P(),
            P(),
            P("tp", None),
            P("ep", "tp", None, None),
            P("ep", "tp", None),
            P("ep", "tp"),
            P(),
            P("ep", None),
            P("ep", None),
            P("ep", None, "tp"),
            P("ep", None, "tp"),
            P("ep", "tp", None),
        ),
        out_specs=(P("ep", None), P("ep", "tp", None, None), P("ep", "tp", None), P("ep", "tp")),
        check_vma=False,
    )
```

```python
import functools

import jax
import jax.numpy as jnp
from jax import lax
from jax.experimental import pallas as pl
from jax.experimental.pallas import tpu as pltpu
from jax.sharding import PartitionSpec as P

EPS = 1e-06
PLANE = 16
FULL_VMEM = 67043328
BF16 = jnp.bfloat16
F32 = jnp.float32


def rms_scaled(values, scales):
    floats = values.astype(F32)
    return floats * lax.rsqrt(jnp.mean(floats * floats, axis=-1, keepdims=True) + EPS) * scales


def place_of(d, nz):
    if d == 0:
        return 0
    return 2 * d - 1 if d <= nz // 2 else 2 * (nz - d)


def moe_kernel(
    nz,
    ng,
    gated_hbm,
    meta_hbm,
    wout_hbm,
    tok_hbm,
    gain_hbm,
    wg_hbm,
    wu_hbm,
    wd_hbm,
    out_ref,
    gated_ref,
    wout,
    tok_ref,
    gain_ref,
    wg,
    wu,
    wd,
    pbuf,
    meta,
    zrows,
    snd,
    rcv,
    osnd0,
    osnd1,
    osnd2,
    back0,
    back1,
    back2,
    zsnd0,
    zsnd1,
    zsnd2,
    zrcv0,
    zrcv1,
    zrcv2,
    hbuf,
    w_sem,
    p_sem,
    m_sem,
    z_sem,
    d_sem,
    b_sem,
    r_sem,
    f_sem,
):
    ep = lax.axis_index("ep")
    tp = lax.axis_index("tp")
    z = ep // ng
    g = ep % ng
    me = g * 2 + tp
    other = 1 - tp
    np_ = 2 * ng
    count, width = tok_ref.shape
    rows, half = zrows.shape[1:]
    per = nz // 2
    slots = 2 * per

    copies = [
        pltpu.make_async_copy(src, dst, w_sem.at[i])
        for i, (src, dst) in enumerate(
            (
                (gated_hbm, gated_ref),
                (wout_hbm, wout),
                (meta_hbm, meta.at[0]),
                (tok_hbm, tok_ref),
                (gain_hbm, gain_ref),
                (wg_hbm, wg),
                (wu_hbm, wu),
                (wd_hbm, wd),
            )
        )
    ]
    weights = copies[5:]
    for copy in copies[:5]:
        copy.start()

    barrier = pltpu.get_barrier_semaphore()

    @pl.loop(1, nz)
    def _(d):
        pl.semaphore_signal(barrier, inc=1, device_id=(lax.rem(z + d, nz) * ng + g, tp))

    @pl.loop(1, np_)
    def _(d):
        q = lax.rem(me + d, np_)
        pl.semaphore_signal(barrier, inc=1, device_id=(z * ng + q // 2, q % 2))

    copies[0].wait()
    copies[1].wait()
    for copy in weights:
        copy.start()
    pbuf[0] = jnp.dot(gated_ref[...], wout[...], preferred_element_type=F32).astype(BF16)
    for copy in copies[2:5]:
        copy.wait()
    pl.semaphore_wait(barrier, nz - 1 + np_ - 1)

    def remote(src, dst, sems, at_src, at_dst, to_ep, to_tp):
        return pltpu.make_async_remote_copy(
            src_ref=src,
            dst_ref=dst,
            send_sem=sems.at[0, at_src],
            recv_sem=sems.at[1, at_dst],
            device_id=(to_ep, to_tp),
        )

    def along_z(sems, source, target, places=range(1, nz)):
        sent, arriving = {}, {}
        for here in places:
            d = [d for d in range(nz) if place_of(d, nz) == here][0]
            there = place_of(nz - d, nz)
            to = lax.rem(z + d, nz) * ng + g
            sent[here] = remote(source(here), target(there), sems, here, there, to, tp)
            arriving[here] = remote(source(here), target(here), sems, here, here, to, tp)
        return sent, arriving

    swap = remote(pbuf.at[0], pbuf.at[1], p_sem, 0, 0, ep, other)
    swap.start()
    meta_out, meta_in = along_z(m_sem, lambda o: meta.at[0], lambda o: meta.at[o])
    for o in range(1, nz):
        meta_out[o].start()

    swap.wait_recv()
    mixed = (pbuf[0].astype(F32) + pbuf[1].astype(F32)).astype(BF16)
    resid = (tok_ref[...].astype(F32) + mixed.astype(F32)).astype(BF16)
    ffn_in = rms_scaled(resid, gain_ref[...]).astype(BF16)

    def my_half(values):
        return jnp.where(tp == 0, values[:, :half], values[:, half:])

    if rows > count:
        zrows[0] = jnp.zeros((rows, half), BF16)
    zrows[0, :count, :] = my_half(ffn_in)
    z_out, z_in = along_z(z_sem, lambda o: zrows.at[0], lambda o: zrows.at[o])
    for o in range(1, nz):
        z_out[o].start()

    for o in range(1, nz):
        meta_in[o].wait_recv()

    first = (z * ng + 1).astype(F32)
    lanes = per * rows
    picks, mixes = [], []
    for c in range(2):
        whole = [
            meta[c * per + i, rows:, :] if i == 0 else pltpu.roll(meta[c * per + i, rows:, :], i * rows, 1)
            for i in range(per)
        ]
        by_lane = whole[0]
        for part in whole[1:]:
            by_lane = by_lane + part
        source = lax.broadcasted_iota(jnp.int32, (4, lanes), 1) // rows
        slot_t = (
            (by_lane[0:4, :lanes] - first) * slots + by_lane[4:8, :lanes]
        ).astype(jnp.int32) + 2 * source
        slot_at = lax.broadcasted_iota(jnp.int32, (ng * slots, lanes), 0)
        pick = jnp.zeros((ng * slots, lanes), F32)
        for k in range(4):
            pick = pick + jnp.where(slot_at == slot_t[k : k + 1, :], 1.0, 0.0)
        picks.append(pick.astype(BF16))
        by_row = meta[c * per : (c + 1) * per, :rows, :].reshape(lanes, meta.shape[2])
        source = lax.broadcasted_iota(jnp.int32, (lanes, 4), 0) // rows
        slot_r = ((by_row[:, 0:4] - first) * slots + by_row[:, 8:12]).astype(jnp.int32) + 2 * source
        slot_at = lax.broadcasted_iota(jnp.int32, (lanes, ng * slots), 1)
        mix = jnp.zeros((lanes, ng * slots), F32)
        for k in range(4):
            mix = mix + jnp.where(slot_at == slot_r[:, k : k + 1], by_row[:, 4 + k : 5 + k], 0.0)
        mix_hi = mix.astype(BF16)
        mixes.append((mix_hi, (mix - mix_hi.astype(F32)).astype(BF16)))

    def d_copy(c, d, at):
        q = lax.rem(me + d, np_)
        to_g, to_tp = q // 2, q % 2
        return remote(
            snd.at[c, to_g],
            rcv.at[c, at % 2, at // 2],
            d_sem.at[c],
            d,
            at,
            z * ng + to_g,
            to_tp,
        )

    for c in range(2):
        for o in range(max(1, c * per), (c + 1) * per):
            z_in[o].wait_recv()
        gathered = zrows[c * per : (c + 1) * per].reshape(lanes, half)
        snd[c] = (
            jnp.dot(picks[c], gathered, preferred_element_type=F32)
            .astype(BF16)
            .reshape(ng, slots, half)
        )

        @pl.loop(1, np_)
        def _(d):
            d_copy(c, d, me).start()

        rcv[c, tp, g] = snd[c, g]

    for copy in weights:
        copy.wait()

    osnd, back = (osnd0, osnd1, osnd2), (back0, back1, back2)
    zsnd, zrcv = (zsnd0, zsnd1, zsnd2), (zrcv0, zrcv1, zrcv2)
    units = [(0, 0, half), (1, 0, half // 2), (1, half // 2, half // 2)]

    def b_copy(u, d, at):
        q = lax.rem(me + d, np_)
        to_g, to_tp = q // 2, q % 2
        return remote(
            osnd[u].at[to_tp, to_g],
            back[u].at[at % 2, at // 2],
            b_sem.at[u],
            d,
            at,
            z * ng + to_g,
            to_tp,
        )

    for c in range(2):

        @pl.loop(1, np_)
        def _(d):
            d_copy(c, d, lax.rem(me + d, np_)).wait_recv()

        left = rcv[c, 0].reshape(ng * slots, half)
        right = rcv[c, 1].reshape(ng * slots, half)

        def both(w):
            return jnp.dot(left, w[:half, :], preferred_element_type=F32) + jnp.dot(
                right, w[half:, :], preferred_element_type=F32
            )

        gate_val = both(wg)
        hidden = (gate_val * jax.nn.sigmoid(gate_val) * both(wu)).astype(BF16)
        for u, (chunk, start, size) in enumerate(units):
            if chunk == c:
                for h in range(2):
                    cols = slice(h * half + start, h * half + start + size)
                    osnd[u][h] = (
                        jnp.dot(hidden, wd[:, cols], preferred_element_type=F32)
                        .astype(BF16)
                        .reshape(ng, slots, size)
                    )

                @pl.loop(1, np_)
                def _(d):
                    b_copy(u, d, me).start()

                back[u][tp, g] = osnd[u][tp, g]

    @pl.loop(1, np_)
    def _(d):
        for c in range(2):
            d_copy(c, d, me).wait_send()

    swap.wait_send()
    for o in range(1, nz):
        meta_out[o].wait_send()
        z_out[o].wait_send()

    summed = []
    for u, (c, start, size) in enumerate(units):
        r_out, _ = along_z(
            r_sem.at[u],
            lambda o: zsnd[u].at[o % per],
            lambda o: zrcv[u].at[o],
            range(max(1, c * per), (c + 1) * per),
        )

        @pl.loop(1, np_)
        def _(d):
            b_copy(u, d, lax.rem(me + d, np_)).wait_recv()

        served = (back[u][0].astype(F32) + back[u][1].astype(F32)).astype(BF16)
        served = served.reshape(ng * slots, size)
        mix_hi, mix_lo = mixes[c]
        sums = jnp.dot(mix_hi, served, preferred_element_type=F32) + jnp.dot(
            mix_lo, served, preferred_element_type=F32
        )
        zsnd[u][...] = sums.astype(BF16).reshape(per, rows, size)
        for o in r_out:
            r_out[o].start()
            summed.append(r_out[o])

    @pl.loop(1, np_)
    def _(d):
        for u in range(3):
            b_copy(u, d, me).wait_send()

    total = my_half(resid).astype(F32) + zsnd[0][0, :count, :].astype(F32)
    for d in range(1, nz):
        here, chunk = place_of(d, nz), place_of(nz - d, nz) // per
        pieces = []
        for u, (c, _, _) in enumerate(units):
            if c == chunk:
                at = zrcv[u].at[here]
                remote(at, at, r_sem.at[u], here, here, ep, other).wait_recv()
                pieces.append(zrcv[u][here, :count, :].astype(F32))
        total = total + (pieces[0] if len(pieces) == 1 else jnp.concatenate(pieces, axis=1))
    mine = total.astype(BF16)
    hbuf[0] = mine
    last = remote(hbuf.at[0], hbuf.at[1], f_sem, 0, 0, ep, other)
    last.start()
    last.wait_recv()
    theirs = hbuf[1]
    out_ref[:, :half] = jnp.where(tp == 0, mine, theirs)
    out_ref[:, half:] = jnp.where(tp == 0, theirs, mine)

    for sent in summed:
        sent.wait_send()
    last.wait_send()


def moe(nz, ng, gated, meta, wout, tok, gain, wg, wu, wd):
    count, width = tok.shape
    rows = meta.shape[0] - 8
    half = width // 2
    vmem = pl.BlockSpec(memory_space=pltpu.VMEM)
    hbm = pl.BlockSpec(memory_space=pltpu.HBM)

    sizes = (half, half // 2, half // 2)

    def sems(*n):
        return pltpu.SemaphoreType.DMA(n)

    return pl.pallas_call(
        functools.partial(moe_kernel, nz, ng),
        out_shape=jax.ShapeDtypeStruct((count, width), BF16),
        in_specs=[hbm] * 8,
        out_specs=vmem,
        scratch_shapes=[pltpu.VMEM(a.shape, a.dtype) for a in (gated, wout, tok, gain, wg, wu, wd)]
        + [
            pltpu.VMEM((2, count, width), BF16),
            pltpu.VMEM((nz, *meta.shape), F32),
            pltpu.VMEM((nz, rows, half), BF16),
            pltpu.VMEM((2, ng, nz, half), BF16),
            pltpu.VMEM((2, 2, ng, nz, half), BF16),
        ]
        + [pltpu.VMEM((2, ng, nz, n), BF16) for n in sizes] * 2
        + [pltpu.VMEM((nz // 2, rows, n), BF16) for n in sizes]
        + [pltpu.VMEM((nz, rows, n), BF16) for n in sizes]
        + [
            pltpu.VMEM((2, count, half), BF16),
            sems(8),
            sems(2, 1),
            sems(2, nz),
            sems(2, nz),
            sems(2, 2, 2 * ng),
            sems(3, 2, 2 * ng),
            sems(3, 2, nz),
            sems(2, 1),
        ],
        compiler_params=pltpu.CompilerParams(
            collective_id=0, has_side_effects=True, vmem_limit_bytes=FULL_VMEM
        ),
        name="experts",
    )(gated, meta, wout, tok, gain, wg, wu, wd)


def cell_kernel(
    tok_hbm,
    ngain_hbm,
    wi_hbm,
    wf_hbm,
    bias_hbm,
    hgain_hbm,
    norm_hbm,
    stab_hbm,
    ids_hbm,
    probs_hbm,
    wq_hbm,
    wk_hbm,
    wv_hbm,
    wo_hbm,
    mem_hbm,
    gated_ref,
    meta_ref,
    nnorm_ref,
    nstab_ref,
    nmem_hbm,
    tok_ref,
    ngain_ref,
    wi_ref,
    wf_ref,
    bias_ref,
    hgain_ref,
    norm_ref,
    stab_ref,
    ids_ref,
    probs_ref,
    wq,
    wk,
    wv,
    wo,
    mem,
    num,
    s_sem,
    w_sem,
    in_sem,
    out_sem,
):
    tp = lax.axis_index("tp")
    count, width = tok_ref.shape
    heads, dim = norm_ref.shape[1:]
    small = [
        pltpu.make_async_copy(src, dst, s_sem.at[i])
        for i, (src, dst) in enumerate(
            (
                (ids_hbm, ids_ref),
                (probs_hbm, probs_ref),
                (tok_hbm, tok_ref),
                (ngain_hbm, ngain_ref),
                (wi_hbm, wi_ref),
                (wf_hbm, wf_ref),
                (bias_hbm, bias_ref),
                (stab_hbm, stab_ref),
                (norm_hbm, norm_ref),
                (hgain_hbm, hgain_ref),
            )
        )
    ]
    loads = [
        pltpu.make_async_copy(src, dst, w_sem.at[i])
        for i, (src, dst) in enumerate(
            ((wk_hbm, wk), (wv_hbm, wv), (wq_hbm, wq), (wo_hbm, wo))
        )
    ]
    reads = [pltpu.make_async_copy(mem_hbm.at[b], mem.at[b], in_sem.at[b]) for b in range(count)]
    writes = [pltpu.make_async_copy(mem.at[b], nmem_hbm.at[b], out_sem.at[b]) for b in range(count)]
    for copy in small + loads[:3]:
        copy.start()

    for copy in small:
        copy.wait()
    ids = ids_ref[...].astype(F32).T.astype(jnp.int32)
    probs = probs_ref[...].T
    weights = probs / jnp.sum(probs, axis=-1, keepdims=True)
    lane = lax.broadcasted_iota(jnp.int32, (count, 128), 1)
    row = lax.broadcasted_iota(jnp.int32, (count, 128), 0)
    top = ids.shape[1]
    named = [lane == ids[:, k : k + 1] for k in range(top)]
    onehot = jnp.zeros((count, 128), F32)
    for k in range(top):
        onehot = onehot + jnp.where(named[k], 1.0, 0.0)
    rows16 = meta_ref.shape[0] - 8
    lower = lax.broadcasted_iota(jnp.int32, (count, count), 0) > lax.broadcasted_iota(
        jnp.int32, (count, count), 1
    )
    earlier = jnp.dot(
        jnp.where(lower, 1.0, 0.0).astype(BF16), onehot.astype(BF16), preferred_element_type=F32
    )
    by_row = jnp.zeros((count, 128), F32)
    meta_ref[...] = jnp.zeros(meta_ref.shape, F32)
    for k in range(top):
        rank = jnp.sum(jnp.where(named[k], earlier, 0.0), axis=1, keepdims=True)
        code = ids[:, k : k + 1].astype(F32) + 1.0
        for at, what in ((k, code), (4 + k, weights[:, k : k + 1]), (8 + k, rank)):
            by_row = jnp.where(lane == at, what, by_row)
        for at, what in ((k, code), (4 + k, rank)):
            meta_ref[rows16 + at : rows16 + at + 1, :] = jnp.sum(
                jnp.where(lane == row, what, 0.0), axis=0, keepdims=True
            )
    meta_ref[:count, :] = by_row

    normed = rms_scaled(tok_ref[...], ngain_ref[...]).astype(BF16)
    across = (((1,), (1,)), ((), ()))
    pre_all = lax.dot_general(normed, wi_ref[...], across, preferred_element_type=F32)
    forget_all = jax.nn.log_sigmoid(
        lax.dot_general(normed, wf_ref[...], across, preferred_element_type=F32) + bias_ref[...]
    )

    def project(i, w):
        loads[i].wait()
        return jnp.dot(normed, w[...], preferred_element_type=F32)

    third = count // 3
    key = project(0, wk) * dim ** (-0.5)
    for copy in reads[:third]:
        copy.start()
    value = project(1, wv)
    for copy in reads[third : 2 * third]:
        copy.start()
    query = project(2, wq)
    for copy in reads[2 * third :] + loads[3:]:
        copy.start()
    query_t = query.T
    stab = stab_ref[...].T
    new_stabs = []
    keeps, values, keys_t, floors = [], [], [], []
    for h in range(heads):
        pre = jnp.where(tp == 0, pre_all[:, h : h + 1], pre_all[:, heads + h : heads + h + 1])
        forget = jnp.where(
            tp == 0, forget_all[:, h : h + 1], forget_all[:, heads + h : heads + h + 1]
        )
        carried = forget + stab[:, h : h + 1]
        new_stab = jnp.maximum(carried, pre)
        new_stabs.append(new_stab)
        keep = jnp.exp(carried - new_stab)
        at = slice(h * dim, (h + 1) * dim)
        written = jnp.exp(pre - new_stab) * key[:, at]
        new_norm = keep * norm_ref[:, h, :] + written
        nnorm_ref[:, h, :] = new_norm
        den = jnp.sum(query[:, at] * new_norm, axis=1, keepdims=True)
        floors.append(jnp.maximum(jnp.abs(den), jnp.exp(-new_stab)))
        keeps.append(jnp.broadcast_to(keep, (count, dim)))
        values.append(value[:, at])
        keys_t.append(written.T)
    heads_at = lax.broadcasted_iota(jnp.int32, (count, heads), 1)
    both_stabs = jnp.broadcast_to(new_stabs[0], (count, heads))
    for h in range(1, heads):
        both_stabs = jnp.where(heads_at == h, new_stabs[h], both_stabs)
    nstab_ref[...] = both_stabs.T
    block = 64
    for b in range(count):
        reads[b].wait()
        for h in range(heads):
            kept = keeps[h][b : b + 1, :]
            added = values[h][b : b + 1, :]
            folded = jnp.zeros((8, dim), F32)
            for d in range(0, dim, block):
                new = kept * mem[b, h, d : d + block, :] + keys_t[h][d : d + block, b : b + 1] * added
                mem[b, h, d : d + block, :] = new
                read = query_t[h * dim + d : h * dim + d + block, b : b + 1] * new
                folded = folded + jnp.sum(read.reshape(block // 8, 8, dim), axis=0)
            num[h, b : b + 1, :] = jnp.sum(folded, axis=0, keepdims=True)
        writes[b].start()
    outgate = project(3, wo)
    local_width = heads * dim
    parts = local_width // 128
    gains = jnp.concatenate(
        [
            jnp.where(tp == 0, hgain_ref[i : i + 1, :], hgain_ref[parts + i : parts + i + 1, :])
            for i in range(parts)
        ],
        axis=1,
    )
    for h in range(heads):
        at = slice(h * dim, (h + 1) * dim)
        readout = num[h] / floors[h]
        scaled = (
            readout
            * lax.rsqrt(jnp.mean(readout * readout, axis=-1, keepdims=True) + EPS)
            * gains[:, at]
        )
        gated_ref[:, at] = (scaled * jax.nn.sigmoid(outgate[:, at])).astype(BF16)
    for copy in writes:
        copy.wait()


def cell(small, weights, memory):
    count, width = small[0].shape
    rows16 = -(-count // 16) * 16
    norm_shape = small[6].shape
    vmem = pl.BlockSpec(memory_space=pltpu.VMEM)
    hbm = pl.BlockSpec(memory_space=pltpu.HBM)
    return pl.pallas_call(
        cell_kernel,
        out_shape=(
            jax.ShapeDtypeStruct((count, weights[0].shape[1]), BF16),
            jax.ShapeDtypeStruct((rows16 + 8, 128), F32),
            jax.ShapeDtypeStruct(norm_shape, F32),
            jax.ShapeDtypeStruct((norm_shape[1], count), F32),
            jax.ShapeDtypeStruct(memory.shape, F32),
        ),
        in_specs=[hbm] * (len(small) + len(weights) + 1),
        out_specs=(vmem, vmem, vmem, vmem, hbm),
        scratch_shapes=[pltpu.VMEM(a.shape, a.dtype) for a in (*small, *weights, memory)]
        + [
            pltpu.VMEM((norm_shape[1], count, norm_shape[2]), F32),
            pltpu.SemaphoreType.DMA((len(small),)),
            pltpu.SemaphoreType.DMA((len(weights),)),
            pltpu.SemaphoreType.DMA((count,)),
            pltpu.SemaphoreType.DMA((count,)),
        ],
        compiler_params=pltpu.CompilerParams(vmem_limit_bytes=FULL_VMEM),
        name="cell",
    )(*small, *weights, memory)


def local(
    tokens,
    norm_gain,
    w_query,
    w_key,
    w_value,
    w_outgate,
    w_input_gate,
    w_forget_gate,
    forget_bias,
    head_gain,
    w_output,
    memory,
    normalizer,
    stabilizer,
    ffn_gain,
    route_ids,
    route_probs,
    expert_gate,
    expert_up,
    expert_down,
):
    ep_count = lax.axis_size("ep")
    ng = min(PLANE, ep_count // 2)
    nz = ep_count // ng
    gated, meta, new_normalizer, new_stab, new_memory = cell(
        (
            tokens,
            norm_gain.reshape(1, -1),
            w_input_gate.T,
            w_forget_gate.T,
            forget_bias.reshape(1, -1),
            head_gain.reshape(-1, 128),
            normalizer,
            stabilizer.T,
            route_ids.T,
            route_probs.T,
        ),
        (w_query, w_key, w_value, w_outgate),
        memory,
    )
    next_tokens = moe(
        nz,
        ng,
        gated,
        meta,
        w_output,
        tokens,
        ffn_gain.reshape(1, -1),
        expert_gate[0],
        expert_up[0],
        expert_down[0],
    )
    return (next_tokens, new_memory, new_normalizer, new_stab.T)


def solution(mesh):
    return jax.shard_map(
        local,
        mesh=mesh,
        in_specs=(
            P("ep", None),
            P(),
            P(None, "tp"),
            P(None, "tp"),
            P(None, "tp"),
            P(None, "tp"),
            P(),
            P(),
            P(),
            P(),
            P("tp", None),
            P("ep", "tp", None, None),
            P("ep", "tp", None),
            P("ep", "tp"),
            P(),
            P("ep", None),
            P("ep", None),
            P("ep", None, "tp"),
            P("ep", None, "tp"),
            P("ep", "tp", None),
        ),
        out_specs=(P("ep", None), P("ep", "tp", None, None), P("ep", "tp", None), P("ep", "tp")),
        check_vma=False,
    )
```

```python
import functools

import jax
import jax.numpy as jnp
from jax import lax
from jax.experimental import pallas as pl
from jax.experimental.pallas import tpu as pltpu
from jax.sharding import PartitionSpec as P

EPS = 1e-06
PLANE = 16
MOST_VMEM = 67043328 - (1 << 20)
BF16 = jnp.bfloat16
F32 = jnp.float32


def rms_scaled(values, scales):
    floats = values.astype(F32)
    return floats * lax.rsqrt(jnp.mean(floats * floats, axis=-1, keepdims=True) + EPS) * scales


def place_of(d, nz):
    if d == 0:
        return 0
    return 2 * d - 1 if d <= nz // 2 else 2 * (nz - d)


def moe_kernel(
    nz,
    ng,
    gated_ref,
    meta_ref,
    wout_hbm,
    tok_hbm,
    gain_hbm,
    wg_hbm,
    wu_hbm,
    wd_hbm,
    out_ref,
    wout,
    tok_ref,
    gain_ref,
    wg,
    wu,
    wd,
    pbuf,
    meta,
    zrows,
    snd,
    rcv,
    osnd0,
    osnd1,
    osnd2,
    back0,
    back1,
    back2,
    zsnd0,
    zsnd1,
    zsnd2,
    zrcv0,
    zrcv1,
    zrcv2,
    hbuf,
    w_sem,
    p_sem,
    m_sem,
    z_sem,
    d_sem,
    b_sem,
    r_sem,
    f_sem,
):
    ep = lax.axis_index("ep")
    tp = lax.axis_index("tp")
    z = ep // ng
    g = ep % ng
    me = g * 2 + tp
    other = 1 - tp
    np_ = 2 * ng
    count, width = tok_ref.shape
    rows, half = zrows.shape[1:]
    per = nz // 2
    slots = 2 * per

    copies = [
        pltpu.make_async_copy(src, dst, w_sem.at[i])
        for i, (src, dst) in enumerate(
            (
                (wout_hbm, wout),
                (tok_hbm, tok_ref),
                (gain_hbm, gain_ref),
                (wg_hbm, wg),
                (wu_hbm, wu),
                (wd_hbm, wd),
            )
        )
    ]
    weights = copies[3:]
    for copy in copies[:3]:
        copy.start()

    barrier = pltpu.get_barrier_semaphore()

    @pl.loop(1, nz)
    def _(d):
        pl.semaphore_signal(barrier, inc=1, device_id=(lax.rem(z + d, nz) * ng + g, tp))

    @pl.loop(1, np_)
    def _(d):
        q = lax.rem(me + d, np_)
        pl.semaphore_signal(barrier, inc=1, device_id=(z * ng + q // 2, q % 2))

    meta[0] = meta_ref[...]
    copies[0].wait()
    for copy in weights:
        copy.start()
    pbuf[0] = jnp.dot(gated_ref[...], wout[...], preferred_element_type=F32).astype(BF16)
    for copy in copies[1:3]:
        copy.wait()
    pl.semaphore_wait(barrier, nz - 1 + np_ - 1)

    def remote(src, dst, sems, at_src, at_dst, to_ep, to_tp):
        return pltpu.make_async_remote_copy(
            src_ref=src,
            dst_ref=dst,
            send_sem=sems.at[0, at_src],
            recv_sem=sems.at[1, at_dst],
            device_id=(to_ep, to_tp),
        )

    def along_z(sems, source, target, places=range(1, nz)):
        sent, arriving = {}, {}
        for here in places:
            d = [d for d in range(nz) if place_of(d, nz) == here][0]
            there = place_of(nz - d, nz)
            to = lax.rem(z + d, nz) * ng + g
            sent[here] = remote(source(here), target(there), sems, here, there, to, tp)
            arriving[here] = remote(source(here), target(here), sems, here, here, to, tp)
        return sent, arriving

    swap = remote(pbuf.at[0], pbuf.at[1], p_sem, 0, 0, ep, other)
    swap.start()
    meta_out, meta_in = along_z(m_sem, lambda o: meta.at[0], lambda o: meta.at[o])
    for o in range(1, nz):
        meta_out[o].start()

    swap.wait_recv()
    mixed = (pbuf[0].astype(F32) + pbuf[1].astype(F32)).astype(BF16)
    resid = (tok_ref[...].astype(F32) + mixed.astype(F32)).astype(BF16)
    ffn_in = rms_scaled(resid, gain_ref[...]).astype(BF16)

    def my_half(values):
        return jnp.where(tp == 0, values[:, :half], values[:, half:])

    if rows > count:
        zrows[0] = jnp.zeros((rows, half), BF16)
    zrows[0, :count, :] = my_half(ffn_in)
    z_out, z_in = along_z(z_sem, lambda o: zrows.at[0], lambda o: zrows.at[o])
    for o in range(1, nz):
        z_out[o].start()

    for o in range(1, nz):
        meta_in[o].wait_recv()

    first = (z * ng + 1).astype(F32)
    lanes = per * rows
    picks, mixes = [], []
    for c in range(2):
        whole = [
            meta[c * per + i, rows:, :] if i == 0 else pltpu.roll(meta[c * per + i, rows:, :], i * rows, 1)
            for i in range(per)
        ]
        by_lane = whole[0]
        for part in whole[1:]:
            by_lane = by_lane + part
        source = lax.broadcasted_iota(jnp.int32, (4, lanes), 1) // rows
        slot_t = (
            (by_lane[0:4, :lanes] - first) * slots + by_lane[4:8, :lanes]
        ).astype(jnp.int32) + 2 * source
        slot_at = lax.broadcasted_iota(jnp.int32, (ng * slots, lanes), 0)
        pick = jnp.zeros((ng * slots, lanes), F32)
        for k in range(4):
            pick = pick + jnp.where(slot_at == slot_t[k : k + 1, :], 1.0, 0.0)
        picks.append(pick.astype(BF16))
        by_row = meta[c * per : (c + 1) * per, :rows, :].reshape(lanes, meta.shape[2])
        source = lax.broadcasted_iota(jnp.int32, (lanes, 4), 0) // rows
        slot_r = ((by_row[:, 0:4] - first) * slots + by_row[:, 8:12]).astype(jnp.int32) + 2 * source
        slot_at = lax.broadcasted_iota(jnp.int32, (lanes, ng * slots), 1)
        mix = jnp.zeros((lanes, ng * slots), F32)
        for k in range(4):
            mix = mix + jnp.where(slot_at == slot_r[:, k : k + 1], by_row[:, 4 + k : 5 + k], 0.0)
        mix_hi = mix.astype(BF16)
        mixes.append((mix_hi, (mix - mix_hi.astype(F32)).astype(BF16)))

    def d_copy(c, d, at):
        q = lax.rem(me + d, np_)
        to_g, to_tp = q // 2, q % 2
        return remote(
            snd.at[c, to_g],
            rcv.at[c, at % 2, at // 2],
            d_sem.at[c],
            d,
            at,
            z * ng + to_g,
            to_tp,
        )

    for c in range(2):
        for o in range(max(1, c * per), (c + 1) * per):
            z_in[o].wait_recv()
        gathered = zrows[c * per : (c + 1) * per].reshape(lanes, half)
        snd[c] = (
            jnp.dot(picks[c], gathered, preferred_element_type=F32)
            .astype(BF16)
            .reshape(ng, slots, half)
        )

        @pl.loop(1, np_)
        def _(d):
            d_copy(c, d, me).start()

        rcv[c, tp, g] = snd[c, g]

    for copy in weights:
        copy.wait()

    osnd, back = (osnd0, osnd1, osnd2), (back0, back1, back2)
    zsnd, zrcv = (zsnd0, zsnd1, zsnd2), (zrcv0, zrcv1, zrcv2)
    units = [(0, 0, half), (1, 0, half // 2), (1, half // 2, half // 2)]

    def b_copy(u, d, at):
        q = lax.rem(me + d, np_)
        to_g, to_tp = q // 2, q % 2
        return remote(
            osnd[u].at[to_tp, to_g],
            back[u].at[at % 2, at // 2],
            b_sem.at[u],
            d,
            at,
            z * ng + to_g,
            to_tp,
        )

    for c in range(2):

        @pl.loop(1, np_)
        def _(d):
            d_copy(c, d, lax.rem(me + d, np_)).wait_recv()

        left = rcv[c, 0].reshape(ng * slots, half)
        right = rcv[c, 1].reshape(ng * slots, half)

        def both(w):
            return jnp.dot(left, w[:half, :], preferred_element_type=F32) + jnp.dot(
                right, w[half:, :], preferred_element_type=F32
            )

        gate_val = both(wg)
        hidden = (gate_val * jax.nn.sigmoid(gate_val) * both(wu)).astype(BF16)
        for u, (chunk, start, size) in enumerate(units):
            if chunk == c:
                for h in range(2):
                    cols = slice(h * half + start, h * half + start + size)
                    osnd[u][h] = (
                        jnp.dot(hidden, wd[:, cols], preferred_element_type=F32)
                        .astype(BF16)
                        .reshape(ng, slots, size)
                    )

                @pl.loop(1, np_)
                def _(d):
                    b_copy(u, d, me).start()

                back[u][tp, g] = osnd[u][tp, g]

    @pl.loop(1, np_)
    def _(d):
        for c in range(2):
            d_copy(c, d, me).wait_send()

    swap.wait_send()
    for o in range(1, nz):
        meta_out[o].wait_send()
        z_out[o].wait_send()

    summed = []
    for u, (c, start, size) in enumerate(units):
        r_out, _ = along_z(
            r_sem.at[u],
            lambda o: zsnd[u].at[o % per],
            lambda o: zrcv[u].at[o],
            range(max(1, c * per), (c + 1) * per),
        )

        @pl.loop(1, np_)
        def _(d):
            b_copy(u, d, lax.rem(me + d, np_)).wait_recv()

        served = (back[u][0].astype(F32) + back[u][1].astype(F32)).astype(BF16)
        served = served.reshape(ng * slots, size)
        mix_hi, mix_lo = mixes[c]
        sums = jnp.dot(mix_hi, served, preferred_element_type=F32) + jnp.dot(
            mix_lo, served, preferred_element_type=F32
        )
        zsnd[u][...] = sums.astype(BF16).reshape(per, rows, size)
        for o in r_out:
            r_out[o].start()
            summed.append(r_out[o])

    @pl.loop(1, np_)
    def _(d):
        for u in range(3):
            b_copy(u, d, me).wait_send()

    total = my_half(resid).astype(F32) + zsnd[0][0, :count, :].astype(F32)
    for d in range(1, nz):
        here, chunk = place_of(d, nz), place_of(nz - d, nz) // per
        pieces = []
        for u, (c, _, _) in enumerate(units):
            if c == chunk:
                at = zrcv[u].at[here]
                remote(at, at, r_sem.at[u], here, here, ep, other).wait_recv()
                pieces.append(zrcv[u][here, :count, :].astype(F32))
        total = total + (pieces[0] if len(pieces) == 1 else jnp.concatenate(pieces, axis=1))
    mine = total.astype(BF16)
    hbuf[0] = mine
    last = remote(hbuf.at[0], hbuf.at[1], f_sem, 0, 0, ep, other)
    last.start()
    last.wait_recv()
    theirs = hbuf[1]
    out_ref[:, :half] = jnp.where(tp == 0, mine, theirs)
    out_ref[:, half:] = jnp.where(tp == 0, theirs, mine)

    for sent in summed:
        sent.wait_send()
    last.wait_send()


def moe(nz, ng, gated, meta, wout, tok, gain, wg, wu, wd):
    count, width = tok.shape
    rows = meta.shape[0] - 8
    half = width // 2
    vmem = pl.BlockSpec(memory_space=pltpu.VMEM)
    hbm = pl.BlockSpec(memory_space=pltpu.HBM)

    sizes = (half, half // 2, half // 2)

    def sems(*n):
        return pltpu.SemaphoreType.DMA(n)

    return pl.pallas_call(
        functools.partial(moe_kernel, nz, ng),
        out_shape=pltpu.VMEM((count, width), BF16),
        in_specs=[vmem] * 2 + [hbm] * 6,
        out_specs=vmem,
        scratch_shapes=[pltpu.VMEM(a.shape, a.dtype) for a in (wout, tok, gain, wg, wu, wd)]
        + [
            pltpu.VMEM((2, count, width), BF16),
            pltpu.VMEM((nz, *meta.shape), F32),
            pltpu.VMEM((nz, rows, half), BF16),
            pltpu.VMEM((2, ng, nz, half), BF16),
            pltpu.VMEM((2, 2, ng, nz, half), BF16),
        ]
        + [pltpu.VMEM((2, ng, nz, n), BF16) for n in sizes] * 2
        + [pltpu.VMEM((nz // 2, rows, n), BF16) for n in sizes]
        + [pltpu.VMEM((nz, rows, n), BF16) for n in sizes]
        + [
            pltpu.VMEM((2, count, half), BF16),
            sems(6),
            sems(2, 1),
            sems(2, nz),
            sems(2, nz),
            sems(2, 2, 2 * ng),
            sems(3, 2, 2 * ng),
            sems(3, 2, nz),
            sems(2, 1),
        ],
        compiler_params=pltpu.CompilerParams(
            collective_id=0, has_side_effects=True, vmem_limit_bytes=MOST_VMEM
        ),
        name="experts",
    )(gated, meta, wout, tok, gain, wg, wu, wd)


def cell_kernel(
    tok_hbm,
    ngain_hbm,
    wi_hbm,
    wf_hbm,
    bias_hbm,
    hgain_hbm,
    norm_hbm,
    stab_hbm,
    ids_hbm,
    probs_hbm,
    wq_hbm,
    wk_hbm,
    wv_hbm,
    wo_hbm,
    mem_hbm,
    gated_ref,
    meta_ref,
    nnorm_hbm,
    nstab_hbm,
    nmem_hbm,
    tok_ref,
    ngain_ref,
    wi_ref,
    wf_ref,
    bias_ref,
    hgain_ref,
    norm_ref,
    stab_ref,
    ids_ref,
    probs_ref,
    wq,
    wk,
    wv,
    wo,
    mem,
    num,
    nnorm_ref,
    nstab_ref,
    o_sem,
    s_sem,
    w_sem,
    in_sem,
    out_sem,
):
    tp = lax.axis_index("tp")
    count, width = tok_ref.shape
    heads, dim = norm_ref.shape[1:]
    small = [
        pltpu.make_async_copy(src, dst, s_sem.at[i])
        for i, (src, dst) in enumerate(
            (
                (ids_hbm, ids_ref),
                (probs_hbm, probs_ref),
                (tok_hbm, tok_ref),
                (ngain_hbm, ngain_ref),
                (wi_hbm, wi_ref),
                (wf_hbm, wf_ref),
                (bias_hbm, bias_ref),
                (stab_hbm, stab_ref),
                (norm_hbm, norm_ref),
                (hgain_hbm, hgain_ref),
            )
        )
    ]
    loads = [
        pltpu.make_async_copy(src, dst, w_sem.at[i])
        for i, (src, dst) in enumerate(
            ((wk_hbm, wk), (wv_hbm, wv), (wq_hbm, wq), (wo_hbm, wo))
        )
    ]
    reads = [pltpu.make_async_copy(mem_hbm.at[b], mem.at[b], in_sem.at[b]) for b in range(count)]
    writes = [pltpu.make_async_copy(mem.at[b], nmem_hbm.at[b], out_sem.at[b]) for b in range(count)]
    third = count // 3
    for copy in small + loads[:3] + reads[:third]:
        copy.start()

    for copy in small:
        copy.wait()
    ids = ids_ref[...].astype(F32).T.astype(jnp.int32)
    probs = probs_ref[...].T
    weights = probs / jnp.sum(probs, axis=-1, keepdims=True)
    lane = lax.broadcasted_iota(jnp.int32, (count, 128), 1)
    row = lax.broadcasted_iota(jnp.int32, (count, 128), 0)
    top = ids.shape[1]
    named = [lane == ids[:, k : k + 1] for k in range(top)]
    onehot = jnp.zeros((count, 128), F32)
    for k in range(top):
        onehot = onehot + jnp.where(named[k], 1.0, 0.0)
    rows16 = meta_ref.shape[0] - 8
    lower = lax.broadcasted_iota(jnp.int32, (count, count), 0) > lax.broadcasted_iota(
        jnp.int32, (count, count), 1
    )
    earlier = jnp.dot(
        jnp.where(lower, 1.0, 0.0).astype(BF16), onehot.astype(BF16), preferred_element_type=F32
    )
    by_row = jnp.zeros((count, 128), F32)
    meta_ref[...] = jnp.zeros(meta_ref.shape, F32)
    for k in range(top):
        rank = jnp.sum(jnp.where(named[k], earlier, 0.0), axis=1, keepdims=True)
        code = ids[:, k : k + 1].astype(F32) + 1.0
        for at, what in ((k, code), (4 + k, weights[:, k : k + 1]), (8 + k, rank)):
            by_row = jnp.where(lane == at, what, by_row)
        for at, what in ((k, code), (4 + k, rank)):
            meta_ref[rows16 + at : rows16 + at + 1, :] = jnp.sum(
                jnp.where(lane == row, what, 0.0), axis=0, keepdims=True
            )
    meta_ref[:count, :] = by_row

    normed = rms_scaled(tok_ref[...], ngain_ref[...]).astype(BF16)
    across = (((1,), (1,)), ((), ()))
    pre_all = lax.dot_general(normed, wi_ref[...], across, preferred_element_type=F32)
    forget_all = jax.nn.log_sigmoid(
        lax.dot_general(normed, wf_ref[...], across, preferred_element_type=F32) + bias_ref[...]
    )

    def project(i, w):
        loads[i].wait()
        return jnp.dot(normed, w[...], preferred_element_type=F32)

    key = project(0, wk) * dim ** (-0.5)
    for copy in reads[third : 2 * third]:
        copy.start()
    value = project(1, wv)
    for copy in reads[2 * third :] + loads[3:]:
        copy.start()
    query = project(2, wq)
    query_t = query.T
    stab = stab_ref[...].T
    new_stabs = []
    keeps, values, keys_t, floors = [], [], [], []
    for h in range(heads):
        pre = jnp.where(tp == 0, pre_all[:, h : h + 1], pre_all[:, heads + h : heads + h + 1])
        forget = jnp.where(
            tp == 0, forget_all[:, h : h + 1], forget_all[:, heads + h : heads + h + 1]
        )
        carried = forget + stab[:, h : h + 1]
        new_stab = jnp.maximum(carried, pre)
        new_stabs.append(new_stab)
        keep = jnp.exp(carried - new_stab)
        at = slice(h * dim, (h + 1) * dim)
        written = jnp.exp(pre - new_stab) * key[:, at]
        new_norm = keep * norm_ref[:, h, :] + written
        nnorm_ref[:, h, :] = new_norm
        den = jnp.sum(query[:, at] * new_norm, axis=1, keepdims=True)
        floors.append(jnp.maximum(jnp.abs(den), jnp.exp(-new_stab)))
        keeps.append(jnp.broadcast_to(keep, (count, dim)))
        key_hi = written.astype(BF16).astype(F32)
        value_hi = value[:, at].astype(BF16).astype(F32)
        keys_t.append(
            jnp.concatenate([key_hi, key_hi, written - key_hi], axis=0).T.astype(BF16)
        )
        values.append(jnp.concatenate([value_hi, value[:, at] - value_hi, value_hi], axis=0))
    heads_at = lax.broadcasted_iota(jnp.int32, (count, heads), 1)
    both_stabs = jnp.broadcast_to(new_stabs[0], (count, heads))
    for h in range(1, heads):
        both_stabs = jnp.where(heads_at == h, new_stabs[h], both_stabs)
    nstab_ref[...] = both_stabs.T
    results = [
        pltpu.make_async_copy(nnorm_ref, nnorm_hbm, o_sem.at[0]),
        pltpu.make_async_copy(nstab_ref, nstab_hbm, o_sem.at[1]),
    ]
    for copy in results:
        copy.start()
    sequence = lax.rem(lax.broadcasted_iota(jnp.int32, (3 * count, dim), 0), count)
    block = 64
    for b in range(count):
        reads[b].wait()
        for h in range(heads):
            kept = keeps[h][b : b + 1, :]
            added = jnp.where(sequence == b, values[h], 0.0).astype(BF16)
            folded = jnp.zeros((8, dim), F32)
            for d in range(0, dim, block):
                new = kept * mem[b, h, d : d + block, :] + jnp.dot(
                    keys_t[h][d : d + block, :], added, preferred_element_type=F32
                )
                mem[b, h, d : d + block, :] = new
                read = query_t[h * dim + d : h * dim + d + block, b : b + 1] * new
                folded = folded + jnp.sum(read.reshape(block // 8, 8, dim), axis=0)
            num[h, b : b + 1, :] = jnp.sum(folded, axis=0, keepdims=True)
        writes[b].start()
    outgate = project(3, wo)
    local_width = heads * dim
    parts = local_width // 128
    gains = jnp.concatenate(
        [
            jnp.where(tp == 0, hgain_ref[i : i + 1, :], hgain_ref[parts + i : parts + i + 1, :])
            for i in range(parts)
        ],
        axis=1,
    )
    for h in range(heads):
        at = slice(h * dim, (h + 1) * dim)
        readout = num[h] / floors[h]
        scaled = (
            readout
            * lax.rsqrt(jnp.mean(readout * readout, axis=-1, keepdims=True) + EPS)
            * gains[:, at]
        )
        gated_ref[:, at] = (scaled * jax.nn.sigmoid(outgate[:, at])).astype(BF16)
    for copy in writes + results:
        copy.wait()


def cell(small, weights, memory):
    count, width = small[0].shape
    rows16 = -(-count // 16) * 16
    norm_shape = small[6].shape
    vmem = pl.BlockSpec(memory_space=pltpu.VMEM)
    hbm = pl.BlockSpec(memory_space=pltpu.HBM)
    return pl.pallas_call(
        cell_kernel,
        out_shape=(
            pltpu.VMEM((count, weights[0].shape[1]), BF16),
            pltpu.VMEM((rows16 + 8, 128), F32),
            jax.ShapeDtypeStruct(norm_shape, F32),
            jax.ShapeDtypeStruct((norm_shape[1], count), F32),
            jax.ShapeDtypeStruct(memory.shape, F32),
        ),
        in_specs=[hbm] * (len(small) + len(weights) + 1),
        out_specs=(vmem, vmem, hbm, hbm, hbm),
        scratch_shapes=[pltpu.VMEM(a.shape, a.dtype) for a in (*small, *weights, memory)]
        + [
            pltpu.VMEM((norm_shape[1], count, norm_shape[2]), F32),
            pltpu.VMEM(norm_shape, F32),
            pltpu.VMEM((norm_shape[1], count), F32),
            pltpu.SemaphoreType.DMA((2,)),
            pltpu.SemaphoreType.DMA((len(small),)),
            pltpu.SemaphoreType.DMA((len(weights),)),
            pltpu.SemaphoreType.DMA((count,)),
            pltpu.SemaphoreType.DMA((count,)),
        ],
        compiler_params=pltpu.CompilerParams(vmem_limit_bytes=MOST_VMEM),
        name="cell",
    )(*small, *weights, memory)


def local(
    tokens,
    norm_gain,
    w_query,
    w_key,
    w_value,
    w_outgate,
    w_input_gate,
    w_forget_gate,
    forget_bias,
    head_gain,
    w_output,
    memory,
    normalizer,
    stabilizer,
    ffn_gain,
    route_ids,
    route_probs,
    expert_gate,
    expert_up,
    expert_down,
):
    ep_count = lax.axis_size("ep")
    ng = min(PLANE, ep_count // 2)
    nz = ep_count // ng
    gated, meta, new_normalizer, new_stab, new_memory = cell(
        (
            tokens,
            norm_gain.reshape(1, -1),
            w_input_gate.T,
            w_forget_gate.T,
            forget_bias.reshape(1, -1),
            head_gain.reshape(-1, 128),
            normalizer,
            stabilizer.T,
            route_ids.T,
            route_probs.T,
        ),
        (w_query, w_key, w_value, w_outgate),
        memory,
    )
    gated = pltpu.with_memory_space_constraint(gated, pltpu.VMEM)
    meta = pltpu.with_memory_space_constraint(meta, pltpu.VMEM)
    next_tokens = moe(
        nz,
        ng,
        gated,
        meta,
        w_output,
        tokens,
        ffn_gain.reshape(1, -1),
        expert_gate[0],
        expert_up[0],
        expert_down[0],
    )
    return (next_tokens, new_memory, new_normalizer, new_stab.T)


def solution(mesh):
    return jax.shard_map(
        local,
        mesh=mesh,
        in_specs=(
            P("ep", None),
            P(),
            P(None, "tp"),
            P(None, "tp"),
            P(None, "tp"),
            P(None, "tp"),
            P(),
            P(),
            P(),
            P(),
            P("tp", None),
            P("ep", "tp", None, None),
            P("ep", "tp", None),
            P("ep", "tp"),
            P(),
            P("ep", None),
            P("ep", None),
            P("ep", None, "tp"),
            P("ep", None, "tp"),
            P("ep", "tp", None),
        ),
        out_specs=(P("ep", None), P("ep", "tp", None, None), P("ep", "tp", None), P("ep", "tp")),
        check_vma=False,
    )
```

```python
import functools

import jax
import jax.numpy as jnp
from jax import lax
from jax.experimental import pallas as pl
from jax.experimental.pallas import tpu as pltpu
from jax.sharding import PartitionSpec as P

EPS = 1e-06
PLANE = 16
MOST_VMEM = 67043328 - (1 << 20)
BF16 = jnp.bfloat16
F32 = jnp.float32


def rms_scaled(values, scales):
    floats = values.astype(F32)
    return floats * lax.rsqrt(jnp.mean(floats * floats, axis=-1, keepdims=True) + EPS) * scales


def place_of(d, nz):
    if d == 0:
        return 0
    return 2 * d - 1 if d <= nz // 2 else 2 * (nz - d)


def moe_kernel(
    nz,
    ng,
    gated_ref,
    meta_ref,
    wout_hbm,
    tok_hbm,
    gain_hbm,
    wg_hbm,
    wu_hbm,
    wd_hbm,
    out_ref,
    wout,
    tok_ref,
    gain_ref,
    wg,
    wu,
    wd,
    pbuf,
    meta,
    zrows,
    snd,
    rcv,
    osnd0,
    osnd1,
    osnd2,
    back0,
    back1,
    back2,
    zsnd0,
    zsnd1,
    zsnd2,
    zrcv0,
    zrcv1,
    zrcv2,
    hbuf,
    w_sem,
    p_sem,
    m_sem,
    z_sem,
    d_sem,
    b_sem,
    r_sem,
    f_sem,
):
    ep = lax.axis_index("ep")
    tp = lax.axis_index("tp")
    z = ep // ng
    g = ep % ng
    me = g * 2 + tp
    other = 1 - tp
    np_ = 2 * ng
    count, width = tok_ref.shape
    rows = meta.shape[1] - 8
    half = width // 2
    per = nz // 2
    slots = 2 * per

    copies = [
        pltpu.make_async_copy(src, dst, w_sem.at[i])
        for i, (src, dst) in enumerate(
            (
                (wout_hbm, wout),
                (tok_hbm, tok_ref),
                (gain_hbm, gain_ref),
                (wg_hbm, wg),
                (wu_hbm, wu),
                (wd_hbm, wd),
            )
        )
    ]
    weights = copies[3:]
    for copy in copies[:3]:
        copy.start()

    barrier = pltpu.get_barrier_semaphore()

    @pl.loop(1, nz)
    def _(d):
        pl.semaphore_signal(barrier, inc=1, device_id=(lax.rem(z + d, nz) * ng + g, tp))

    @pl.loop(1, np_)
    def _(d):
        q = lax.rem(me + d, np_)
        pl.semaphore_signal(barrier, inc=1, device_id=(z * ng + q // 2, q % 2))

    meta[0] = meta_ref[...]
    copies[0].wait()
    for copy in weights:
        copy.start()
    pbuf[0] = jnp.dot(gated_ref[...], wout[...], preferred_element_type=F32).astype(BF16)
    for copy in copies[1:3]:
        copy.wait()
    pl.semaphore_wait(barrier, nz - 1 + np_ - 1)

    def remote(src, dst, sems, at_src, at_dst, to_ep, to_tp):
        return pltpu.make_async_remote_copy(
            src_ref=src,
            dst_ref=dst,
            send_sem=sems.at[0, at_src],
            recv_sem=sems.at[1, at_dst],
            device_id=(to_ep, to_tp),
        )

    def along_z(sems, source, target, places=range(1, nz)):
        sent, arriving = {}, {}
        for here in places:
            d = [d for d in range(nz) if place_of(d, nz) == here][0]
            there = place_of(nz - d, nz)
            to = lax.rem(z + d, nz) * ng + g
            sent[here] = remote(source(here), target(there), sems, here, there, to, tp)
            arriving[here] = remote(source(here), target(here), sems, here, here, to, tp)
        return sent, arriving

    swap = remote(pbuf.at[0], pbuf.at[1], p_sem, 0, 0, ep, other)
    swap.start()
    meta_out, meta_in = along_z(m_sem, lambda o: meta.at[0], lambda o: meta.at[o])
    for o in range(1, nz):
        meta_out[o].start()

    swap.wait_recv()
    mixed = (pbuf[0].astype(F32) + pbuf[1].astype(F32)).astype(BF16)
    resid = (tok_ref[...].astype(F32) + mixed.astype(F32)).astype(BF16)
    ffn_in = rms_scaled(resid, gain_ref[...]).astype(BF16)

    def my_half(values):
        return jnp.where(tp == 0, values[:, :half], values[:, half:])

    def stacked(values):
        n = values.shape[1] // 4
        quarters = [values[:, q * n : (q + 1) * n] for q in range(4)]
        return jnp.concatenate(quarters, axis=0).astype(BF16)

    def unstacked(values):
        floats = values.astype(F32)
        return jnp.concatenate([floats[q * count : (q + 1) * count] for q in range(4)], axis=1)

    zrows[0] = stacked(my_half(ffn_in.astype(F32)))
    z_out, z_in = along_z(z_sem, lambda o: zrows.at[0], lambda o: zrows.at[o])
    for o in range(1, nz):
        z_out[o].start()

    for o in range(1, nz):
        meta_in[o].wait_recv()

    first = (z * ng + 1).astype(F32)
    lanes = per * rows
    picks, mixes = [], []
    for c in range(2):
        by_lane = jnp.concatenate(
            [meta[c * per + i, rows:, : 4 * count] for i in range(per)], axis=1
        )
        lane = lax.broadcasted_iota(jnp.int32, (4, 4 * count * per), 1)
        slot_t = ((by_lane[0:4] - first) * slots + by_lane[4:8]).astype(jnp.int32) + 2 * (
            lane // (4 * count)
        )
        slot_at = lax.broadcasted_iota(jnp.int32, (ng * slots, 4 * count * per), 0)
        pick = jnp.zeros((ng * slots, 4 * count * per), F32)
        for k in range(4):
            pick = pick + jnp.where(slot_at == slot_t[k : k + 1, :], 1.0, 0.0)
        quarter = lax.rem(lax.broadcasted_iota(jnp.int32, pick.shape, 1), 4 * count) // count
        picks.append([jnp.where(quarter == q, pick, 0.0).astype(BF16) for q in range(4)])
        by_row = meta[c * per : (c + 1) * per, :rows, :].reshape(lanes, meta.shape[2])
        source = lax.broadcasted_iota(jnp.int32, (lanes, 4), 0) // rows
        slot_r = ((by_row[:, 0:4] - first) * slots + by_row[:, 8:12]).astype(jnp.int32) + 2 * source
        slot_at = lax.broadcasted_iota(jnp.int32, (lanes, ng * slots), 1)
        mix = jnp.zeros((lanes, ng * slots), F32)
        for k in range(4):
            mix = mix + jnp.where(slot_at == slot_r[:, k : k + 1], by_row[:, 4 + k : 5 + k], 0.0)
        mix_hi = mix.astype(BF16)
        mixes.append((mix_hi, (mix - mix_hi.astype(F32)).astype(BF16)))

    def d_copy(c, d, at):
        q = lax.rem(me + d, np_)
        to_g, to_tp = q // 2, q % 2
        return remote(
            snd.at[c, to_g],
            rcv.at[c, at % 2, at // 2],
            d_sem.at[c],
            d,
            at,
            z * ng + to_g,
            to_tp,
        )

    for c in range(2):
        for o in range(max(1, c * per), (c + 1) * per):
            z_in[o].wait_recv()
        gathered = zrows[c * per : (c + 1) * per].reshape(4 * count * per, half // 4)
        for q in range(4):
            snd[c, :, :, q * (half // 4) : (q + 1) * (half // 4)] = (
                jnp.dot(picks[c][q], gathered, preferred_element_type=F32)
                .astype(BF16)
                .reshape(ng, slots, half // 4)
            )

        @pl.loop(1, np_)
        def _(d):
            d_copy(c, d, me).start()

        rcv[c, tp, g] = snd[c, g]

    for copy in weights:
        copy.wait()

    osnd, back = (osnd0, osnd1, osnd2), (back0, back1, back2)
    zsnd, zrcv = (zsnd0, zsnd1, zsnd2), (zrcv0, zrcv1, zrcv2)
    units = [(0, 0, half), (1, 0, half // 2), (1, half // 2, half // 2)]

    def b_copy(u, d, at):
        q = lax.rem(me + d, np_)
        to_g, to_tp = q // 2, q % 2
        return remote(
            osnd[u].at[to_tp, to_g],
            back[u].at[at % 2, at // 2],
            b_sem.at[u],
            d,
            at,
            z * ng + to_g,
            to_tp,
        )

    for c in range(2):

        @pl.loop(1, np_)
        def _(d):
            d_copy(c, d, lax.rem(me + d, np_)).wait_recv()

        left = rcv[c, 0].reshape(ng * slots, half)
        right = rcv[c, 1].reshape(ng * slots, half)

        def both(w):
            return jnp.dot(left, w[:half, :], preferred_element_type=F32) + jnp.dot(
                right, w[half:, :], preferred_element_type=F32
            )

        gate_val = both(wg)
        hidden = (gate_val * jax.nn.sigmoid(gate_val) * both(wu)).astype(BF16)
        for u, (chunk, start, size) in enumerate(units):
            if chunk == c:
                for h in range(2):
                    cols = slice(h * half + start, h * half + start + size)
                    osnd[u][h] = (
                        jnp.dot(hidden, wd[:, cols], preferred_element_type=F32)
                        .astype(BF16)
                        .reshape(ng, slots, size)
                    )

                @pl.loop(1, np_)
                def _(d):
                    b_copy(u, d, me).start()

                back[u][tp, g] = osnd[u][tp, g]

    @pl.loop(1, np_)
    def _(d):
        for c in range(2):
            d_copy(c, d, me).wait_send()

    swap.wait_send()
    for o in range(1, nz):
        meta_out[o].wait_send()
        z_out[o].wait_send()

    summed = []
    for u, (c, start, size) in enumerate(units):
        r_out, _ = along_z(
            r_sem.at[u],
            lambda o: zsnd[u].at[o % per],
            lambda o: zrcv[u].at[o],
            range(max(1, c * per), (c + 1) * per),
        )

        @pl.loop(1, np_)
        def _(d):
            b_copy(u, d, lax.rem(me + d, np_)).wait_recv()

        served = (back[u][0].astype(F32) + back[u][1].astype(F32)).astype(BF16)
        served = served.reshape(ng * slots, size)
        mix_hi, mix_lo = mixes[c]
        sums = jnp.dot(mix_hi, served, preferred_element_type=F32) + jnp.dot(
            mix_lo, served, preferred_element_type=F32
        )
        for o in range(per):
            zsnd[u][o] = stacked(sums[o * rows : o * rows + count])
        for o in r_out:
            r_out[o].start()
            summed.append(r_out[o])

    @pl.loop(1, np_)
    def _(d):
        for u in range(3):
            b_copy(u, d, me).wait_send()

    total = my_half(resid).astype(F32) + unstacked(zsnd[0][0])
    for d in range(1, nz):
        here, chunk = place_of(d, nz), place_of(nz - d, nz) // per
        pieces = []
        for u, (c, _, _) in enumerate(units):
            if c == chunk:
                at = zrcv[u].at[here]
                remote(at, at, r_sem.at[u], here, here, ep, other).wait_recv()
                pieces.append(unstacked(zrcv[u][here]))
        total = total + (pieces[0] if len(pieces) == 1 else jnp.concatenate(pieces, axis=1))
    mine = total.astype(BF16)
    hbuf[0] = mine
    last = remote(hbuf.at[0], hbuf.at[1], f_sem, 0, 0, ep, other)
    last.start()
    last.wait_recv()
    theirs = hbuf[1]
    out_ref[:, :half] = jnp.where(tp == 0, mine, theirs)
    out_ref[:, half:] = jnp.where(tp == 0, theirs, mine)

    for sent in summed:
        sent.wait_send()
    last.wait_send()


def moe(nz, ng, gated, meta, wout, tok, gain, wg, wu, wd):
    count, width = tok.shape
    half = width // 2
    vmem = pl.BlockSpec(memory_space=pltpu.VMEM)
    hbm = pl.BlockSpec(memory_space=pltpu.HBM)

    sizes = (half, half // 2, half // 2)

    def sems(*n):
        return pltpu.SemaphoreType.DMA(n)

    return pl.pallas_call(
        functools.partial(moe_kernel, nz, ng),
        out_shape=pltpu.VMEM((count, width), BF16),
        in_specs=[vmem] * 2 + [hbm] * 6,
        out_specs=vmem,
        scratch_shapes=[pltpu.VMEM(a.shape, a.dtype) for a in (wout, tok, gain, wg, wu, wd)]
        + [
            pltpu.VMEM((2, count, width), BF16),
            pltpu.VMEM((nz, *meta.shape), F32),
            pltpu.VMEM((nz, 4 * count, half // 4), BF16),
            pltpu.VMEM((2, ng, nz, half), BF16),
            pltpu.VMEM((2, 2, ng, nz, half), BF16),
        ]
        + [pltpu.VMEM((2, ng, nz, n), BF16) for n in sizes] * 2
        + [pltpu.VMEM((nz // 2, 4 * count, n // 4), BF16) for n in sizes]
        + [pltpu.VMEM((nz, 4 * count, n // 4), BF16) for n in sizes]
        + [
            pltpu.VMEM((2, count, half), BF16),
            sems(6),
            sems(2, 1),
            sems(2, nz),
            sems(2, nz),
            sems(2, 2, 2 * ng),
            sems(3, 2, 2 * ng),
            sems(3, 2, nz),
            sems(2, 1),
        ],
        compiler_params=pltpu.CompilerParams(
            collective_id=0, has_side_effects=True, vmem_limit_bytes=MOST_VMEM
        ),
        name="experts",
    )(gated, meta, wout, tok, gain, wg, wu, wd)


def cell_kernel(
    tok_hbm,
    ngain_hbm,
    wi_hbm,
    wf_hbm,
    bias_hbm,
    hgain_hbm,
    norm_hbm,
    stab_hbm,
    ids_hbm,
    probs_hbm,
    wq_hbm,
    wk_hbm,
    wv_hbm,
    wo_hbm,
    mem_hbm,
    gated_ref,
    meta_ref,
    nnorm_hbm,
    nstab_hbm,
    nmem_hbm,
    tok_ref,
    ngain_ref,
    wi_ref,
    wf_ref,
    bias_ref,
    hgain_ref,
    norm_ref,
    stab_ref,
    ids_ref,
    probs_ref,
    wq,
    wk,
    wv,
    wo,
    mem,
    num,
    nnorm_ref,
    nstab_ref,
    o_sem,
    s_sem,
    w_sem,
    in_sem,
    out_sem,
):
    tp = lax.axis_index("tp")
    count, width = tok_ref.shape
    heads, dim = norm_ref.shape[1:]
    small = [
        pltpu.make_async_copy(src, dst, s_sem.at[i])
        for i, (src, dst) in enumerate(
            (
                (ids_hbm, ids_ref),
                (probs_hbm, probs_ref),
                (tok_hbm, tok_ref),
                (ngain_hbm, ngain_ref),
                (wi_hbm, wi_ref),
                (wf_hbm, wf_ref),
                (bias_hbm, bias_ref),
                (stab_hbm, stab_ref),
                (norm_hbm, norm_ref),
                (hgain_hbm, hgain_ref),
            )
        )
    ]
    loads = [
        pltpu.make_async_copy(src, dst, w_sem.at[i])
        for i, (src, dst) in enumerate(
            ((wk_hbm, wk), (wv_hbm, wv), (wq_hbm, wq), (wo_hbm, wo))
        )
    ]
    reads = [pltpu.make_async_copy(mem_hbm.at[b], mem.at[b], in_sem.at[b]) for b in range(count)]
    writes = [pltpu.make_async_copy(mem.at[b], nmem_hbm.at[b], out_sem.at[b]) for b in range(count)]
    third = count // 3
    for copy in small + loads[:3] + reads[:third]:
        copy.start()

    for copy in small:
        copy.wait()
    ids = ids_ref[...].astype(F32).T.astype(jnp.int32)
    probs = probs_ref[...].T
    weights = probs / jnp.sum(probs, axis=-1, keepdims=True)
    lane = lax.broadcasted_iota(jnp.int32, (count, 128), 1)
    row = lax.broadcasted_iota(jnp.int32, (count, 128), 0)
    top = ids.shape[1]
    named = [lane == ids[:, k : k + 1] for k in range(top)]
    onehot = jnp.zeros((count, 128), F32)
    for k in range(top):
        onehot = onehot + jnp.where(named[k], 1.0, 0.0)
    rows16 = meta_ref.shape[0] - 8
    lower = lax.broadcasted_iota(jnp.int32, (count, count), 0) > lax.broadcasted_iota(
        jnp.int32, (count, count), 1
    )
    earlier = jnp.dot(
        jnp.where(lower, 1.0, 0.0).astype(BF16), onehot.astype(BF16), preferred_element_type=F32
    )
    by_row = jnp.zeros((count, 128), F32)
    meta_ref[...] = jnp.zeros(meta_ref.shape, F32)
    for k in range(top):
        rank = jnp.sum(jnp.where(named[k], earlier, 0.0), axis=1, keepdims=True)
        code = ids[:, k : k + 1].astype(F32) + 1.0
        for at, what in ((k, code), (4 + k, weights[:, k : k + 1]), (8 + k, rank)):
            by_row = jnp.where(lane == at, what, by_row)
        for at, what in ((k, code), (4 + k, rank)):
            meta_ref[rows16 + at : rows16 + at + 1, :] = jnp.sum(
                jnp.where(lax.rem(lane, count) == row, what, 0.0), axis=0, keepdims=True
            )
    meta_ref[:count, :] = by_row

    normed = rms_scaled(tok_ref[...], ngain_ref[...]).astype(BF16)
    across = (((1,), (1,)), ((), ()))
    pre_all = lax.dot_general(normed, wi_ref[...], across, preferred_element_type=F32)
    forget_all = jax.nn.log_sigmoid(
        lax.dot_general(normed, wf_ref[...], across, preferred_element_type=F32) + bias_ref[...]
    )

    def project(i, w):
        loads[i].wait()
        return jnp.dot(normed, w[...], preferred_element_type=F32)

    key = project(0, wk) * dim ** (-0.5)
    for copy in reads[third : 2 * third]:
        copy.start()
    value = project(1, wv)
    for copy in reads[2 * third :] + loads[3:]:
        copy.start()
    query = project(2, wq)
    query_t = query.T
    stab = stab_ref[...].T
    new_stabs = []
    keeps, values, keys_t, floors = [], [], [], []
    for h in range(heads):
        pre = jnp.where(tp == 0, pre_all[:, h : h + 1], pre_all[:, heads + h : heads + h + 1])
        forget = jnp.where(
            tp == 0, forget_all[:, h : h + 1], forget_all[:, heads + h : heads + h + 1]
        )
        carried = forget + stab[:, h : h + 1]
        new_stab = jnp.maximum(carried, pre)
        new_stabs.append(new_stab)
        keep = jnp.exp(carried - new_stab)
        at = slice(h * dim, (h + 1) * dim)
        written = jnp.exp(pre - new_stab) * key[:, at]
        new_norm = keep * norm_ref[:, h, :] + written
        nnorm_ref[:, h, :] = new_norm
        den = jnp.sum(query[:, at] * new_norm, axis=1, keepdims=True)
        floors.append(jnp.maximum(jnp.abs(den), jnp.exp(-new_stab)))
        keeps.append(jnp.broadcast_to(keep, (count, dim)))
        key_hi = written.astype(BF16).astype(F32)
        value_hi = value[:, at].astype(BF16).astype(F32)
        keys_t.append(
            jnp.concatenate([key_hi, key_hi, written - key_hi], axis=0).T.astype(BF16)
        )
        values.append(jnp.concatenate([value_hi, value[:, at] - value_hi, value_hi], axis=0))
    heads_at = lax.broadcasted_iota(jnp.int32, (count, heads), 1)
    both_stabs = jnp.broadcast_to(new_stabs[0], (count, heads))
    for h in range(1, heads):
        both_stabs = jnp.where(heads_at == h, new_stabs[h], both_stabs)
    nstab_ref[...] = both_stabs.T
    results = [
        pltpu.make_async_copy(nnorm_ref, nnorm_hbm, o_sem.at[0]),
        pltpu.make_async_copy(nstab_ref, nstab_hbm, o_sem.at[1]),
    ]
    for copy in results:
        copy.start()
    sequence = lax.rem(lax.broadcasted_iota(jnp.int32, (3 * count, dim), 0), count)
    block = 96
    for b in range(count):
        reads[b].wait()
        for h in range(heads):
            kept = keeps[h][b : b + 1, :]
            added = jnp.where(sequence == b, values[h], 0.0).astype(BF16)
            folded = jnp.zeros((8, dim), F32)
            for d in range(0, dim, block):
                new = kept * mem[b, h, d : d + block, :] + jnp.dot(
                    keys_t[h][d : d + block, :], added, preferred_element_type=F32
                )
                mem[b, h, d : d + block, :] = new
                read = query_t[h * dim + d : h * dim + d + block, b : b + 1] * new
                folded = folded + jnp.sum(read.reshape(block // 8, 8, dim), axis=0)
            num[h, b : b + 1, :] = jnp.sum(folded, axis=0, keepdims=True)
        writes[b].start()
    outgate = project(3, wo)
    local_width = heads * dim
    parts = local_width // 128
    gains = jnp.concatenate(
        [
            jnp.where(tp == 0, hgain_ref[i : i + 1, :], hgain_ref[parts + i : parts + i + 1, :])
            for i in range(parts)
        ],
        axis=1,
    )
    for h in range(heads):
        at = slice(h * dim, (h + 1) * dim)
        readout = num[h] / floors[h]
        scaled = (
            readout
            * lax.rsqrt(jnp.mean(readout * readout, axis=-1, keepdims=True) + EPS)
            * gains[:, at]
        )
        gated_ref[:, at] = (scaled * jax.nn.sigmoid(outgate[:, at])).astype(BF16)
    for copy in writes + results:
        copy.wait()


def cell(small, weights, memory):
    count, width = small[0].shape
    rows16 = -(-count // 16) * 16
    norm_shape = small[6].shape
    vmem = pl.BlockSpec(memory_space=pltpu.VMEM)
    hbm = pl.BlockSpec(memory_space=pltpu.HBM)
    return pl.pallas_call(
        cell_kernel,
        out_shape=(
            pltpu.VMEM((count, weights[0].shape[1]), BF16),
            pltpu.VMEM((rows16 + 8, 128), F32),
            jax.ShapeDtypeStruct(norm_shape, F32),
            jax.ShapeDtypeStruct((norm_shape[1], count), F32),
            jax.ShapeDtypeStruct(memory.shape, F32),
        ),
        in_specs=[hbm] * (len(small) + len(weights) + 1),
        out_specs=(vmem, vmem, hbm, hbm, hbm),
        scratch_shapes=[pltpu.VMEM(a.shape, a.dtype) for a in (*small, *weights, memory)]
        + [
            pltpu.VMEM((norm_shape[1], count, norm_shape[2]), F32),
            pltpu.VMEM(norm_shape, F32),
            pltpu.VMEM((norm_shape[1], count), F32),
            pltpu.SemaphoreType.DMA((2,)),
            pltpu.SemaphoreType.DMA((len(small),)),
            pltpu.SemaphoreType.DMA((len(weights),)),
            pltpu.SemaphoreType.DMA((count,)),
            pltpu.SemaphoreType.DMA((count,)),
        ],
        compiler_params=pltpu.CompilerParams(vmem_limit_bytes=MOST_VMEM),
        name="cell",
    )(*small, *weights, memory)


def local(
    tokens,
    norm_gain,
    w_query,
    w_key,
    w_value,
    w_outgate,
    w_input_gate,
    w_forget_gate,
    forget_bias,
    head_gain,
    w_output,
    memory,
    normalizer,
    stabilizer,
    ffn_gain,
    route_ids,
    route_probs,
    expert_gate,
    expert_up,
    expert_down,
):
    ep_count = lax.axis_size("ep")
    ng = min(PLANE, ep_count // 2)
    nz = ep_count // ng
    gated, meta, new_normalizer, new_stab, new_memory = cell(
        (
            tokens,
            norm_gain.reshape(1, -1),
            w_input_gate.T,
            w_forget_gate.T,
            forget_bias.reshape(1, -1),
            head_gain.reshape(-1, 128),
            normalizer,
            stabilizer.T,
            route_ids.T,
            route_probs.T,
        ),
        (w_query, w_key, w_value, w_outgate),
        memory,
    )
    gated = pltpu.with_memory_space_constraint(gated, pltpu.VMEM)
    meta = pltpu.with_memory_space_constraint(meta, pltpu.VMEM)
    next_tokens = moe(
        nz,
        ng,
        gated,
        meta,
        w_output,
        tokens,
        ffn_gain.reshape(1, -1),
        expert_gate[0],
        expert_up[0],
        expert_down[0],
    )
    return (next_tokens, new_memory, new_normalizer, new_stab.T)


def solution(mesh):
    return jax.shard_map(
        local,
        mesh=mesh,
        in_specs=(
            P("ep", None),
            P(),
            P(None, "tp"),
            P(None, "tp"),
            P(None, "tp"),
            P(None, "tp"),
            P(),
            P(),
            P(),
            P(),
            P("tp", None),
            P("ep", "tp", None, None),
            P("ep", "tp", None),
            P("ep", "tp"),
            P(),
            P("ep", None),
            P("ep", None),
            P("ep", None, "tp"),
            P("ep", None, "tp"),
            P("ep", "tp", None),
        ),
        out_specs=(P("ep", None), P("ep", "tp", None, None), P("ep", "tp", None), P("ep", "tp")),
        check_vma=False,
    )
```

```python
import functools

import jax
import jax.numpy as jnp
from jax import lax
from jax.experimental import pallas as pl
from jax.experimental.pallas import tpu as pltpu
from jax.sharding import PartitionSpec as P

EPS = 1e-06
PLANE = 16
MOST_VMEM = 67043328 - (1 << 20)
BF16 = jnp.bfloat16
F32 = jnp.float32


def rms_scaled(values, scales):
    floats = values.astype(F32)
    return floats * lax.rsqrt(jnp.mean(floats * floats, axis=-1, keepdims=True) + EPS) * scales


def place_of(d, nz):
    if d == 0:
        return 0
    return 2 * d - 1 if d <= nz // 2 else 2 * (nz - d)


def moe_kernel(
    nz,
    ng,
    gated_ref,
    meta_ref,
    wout_hbm,
    tok_hbm,
    gain_hbm,
    wg_hbm,
    wu_hbm,
    wd_hbm,
    out_ref,
    wout,
    tok_ref,
    gain_ref,
    wg,
    wu,
    wd,
    pbuf,
    meta,
    zrows,
    snd,
    rcv,
    osnd0,
    osnd1,
    osnd2,
    back0,
    back1,
    back2,
    zsnd0,
    zsnd1,
    zsnd2,
    zrcv0,
    zrcv1,
    zrcv2,
    hbuf,
    w_sem,
    p_sem,
    m_sem,
    z_sem,
    d_sem,
    b_sem,
    r_sem,
    f_sem,
):
    ep = lax.axis_index("ep")
    tp = lax.axis_index("tp")
    z = ep // ng
    g = ep % ng
    me = g * 2 + tp
    other = 1 - tp
    np_ = 2 * ng
    count, width = tok_ref.shape
    rows = meta.shape[1] - 8
    half = width // 2
    per = nz // 2
    slots = 2 * per

    copies = [
        pltpu.make_async_copy(src, dst, w_sem.at[i])
        for i, (src, dst) in enumerate(
            (
                (wout_hbm, wout),
                (tok_hbm, tok_ref),
                (gain_hbm, gain_ref),
                (wg_hbm, wg),
                (wu_hbm, wu),
                (wd_hbm, wd),
            )
        )
    ]
    weights = copies[3:]
    for copy in copies[:3]:
        copy.start()

    barrier = pltpu.get_barrier_semaphore()

    @pl.loop(1, nz)
    def _(d):
        pl.semaphore_signal(barrier, inc=1, device_id=(lax.rem(z + d, nz) * ng + g, tp))

    @pl.loop(1, np_)
    def _(d):
        q = lax.rem(me + d, np_)
        pl.semaphore_signal(barrier, inc=1, device_id=(z * ng + q // 2, q % 2))

    meta[0] = meta_ref[...]
    copies[0].wait()
    for copy in weights:
        copy.start()
    pbuf[0] = jnp.dot(gated_ref[...], wout[...], preferred_element_type=F32).astype(BF16)
    for copy in copies[1:3]:
        copy.wait()
    pl.semaphore_wait(barrier, nz - 1 + np_ - 1)

    def remote(src, dst, sems, at_src, at_dst, to_ep, to_tp):
        return pltpu.make_async_remote_copy(
            src_ref=src,
            dst_ref=dst,
            send_sem=sems.at[0, at_src],
            recv_sem=sems.at[1, at_dst],
            device_id=(to_ep, to_tp),
        )

    def along_z(sems, source, target, places=range(1, nz)):
        sent, arriving = {}, {}
        for here in places:
            d = [d for d in range(nz) if place_of(d, nz) == here][0]
            there = place_of(nz - d, nz)
            to = lax.rem(z + d, nz) * ng + g
            sent[here] = remote(source(here), target(there), sems, here, there, to, tp)
            arriving[here] = remote(source(here), target(here), sems, here, here, to, tp)
        return sent, arriving

    swap = remote(pbuf.at[0], pbuf.at[1], p_sem, 0, 0, ep, other)
    swap.start()
    meta_out, meta_in = along_z(m_sem, lambda o: meta.at[0], lambda o: meta.at[o])
    for o in range(1, nz):
        meta_out[o].start()

    swap.wait_recv()
    mixed = (pbuf[0].astype(F32) + pbuf[1].astype(F32)).astype(BF16)
    resid = (tok_ref[...].astype(F32) + mixed.astype(F32)).astype(BF16)
    ffn_in = rms_scaled(resid, gain_ref[...]).astype(BF16)

    def my_half(values):
        return jnp.where(tp == 0, values[:, :half], values[:, half:])

    def stacked(values):
        n = values.shape[1] // 4
        quarters = [values[:, q * n : (q + 1) * n] for q in range(4)]
        return jnp.concatenate(quarters, axis=0).astype(BF16)

    def unstacked(values):
        floats = values.astype(F32)
        return jnp.concatenate([floats[q * count : (q + 1) * count] for q in range(4)], axis=1)

    zrows[0] = stacked(my_half(ffn_in.astype(F32)))
    z_out, z_in = along_z(z_sem, lambda o: zrows.at[0], lambda o: zrows.at[o])
    for o in range(1, nz):
        z_out[o].start()

    for o in range(1, nz):
        meta_in[o].wait_recv()

    first = (z * ng + 1).astype(F32)
    lanes = per * rows
    picks, mixes = [], []
    for c in range(2):
        by_lane = jnp.concatenate(
            [meta[c * per + i, rows:, : 4 * count] for i in range(per)], axis=1
        )
        lane = lax.broadcasted_iota(jnp.int32, (4, 4 * count * per), 1)
        slot_t = ((by_lane[0:4] - first) * slots + by_lane[4:8]).astype(jnp.int32) + 2 * (
            lane // (4 * count)
        )
        slot_at = lax.broadcasted_iota(jnp.int32, (ng * slots, 4 * count * per), 0)
        pick = jnp.zeros((ng * slots, 4 * count * per), F32)
        for k in range(4):
            pick = pick + jnp.where(slot_at == slot_t[k : k + 1, :], 1.0, 0.0)
        quarter = lax.rem(lax.broadcasted_iota(jnp.int32, pick.shape, 1), 4 * count) // count
        picks.append([jnp.where(quarter == q, pick, 0.0).astype(BF16) for q in range(4)])
        by_row = meta[c * per : (c + 1) * per, :rows, :].reshape(lanes, meta.shape[2])
        source = lax.broadcasted_iota(jnp.int32, (lanes, 4), 0) // rows
        slot_r = ((by_row[:, 0:4] - first) * slots + by_row[:, 8:12]).astype(jnp.int32) + 2 * source
        slot_at = lax.broadcasted_iota(jnp.int32, (lanes, ng * slots), 1)
        mix = jnp.zeros((lanes, ng * slots), F32)
        for k in range(4):
            mix = mix + jnp.where(slot_at == slot_r[:, k : k + 1], by_row[:, 4 + k : 5 + k], 0.0)
        mix_hi = mix.astype(BF16)
        mixes.append((mix_hi, (mix - mix_hi.astype(F32)).astype(BF16)))

    def d_copy(c, d, at):
        q = lax.rem(me + d, np_)
        to_g, to_tp = q // 2, q % 2
        return remote(
            snd.at[c, to_g],
            rcv.at[c, at % 2, at // 2],
            d_sem.at[c],
            d,
            at,
            z * ng + to_g,
            to_tp,
        )

    for c in range(2):
        for o in range(max(1, c * per), (c + 1) * per):
            z_in[o].wait_recv()
        gathered = zrows[c * per : (c + 1) * per].reshape(4 * count * per, half // 4)
        for q in range(4):
            snd[c, :, :, q * (half // 4) : (q + 1) * (half // 4)] = (
                jnp.dot(picks[c][q], gathered, preferred_element_type=F32)
                .astype(BF16)
                .reshape(ng, slots, half // 4)
            )

        @pl.loop(1, np_)
        def _(d):
            d_copy(c, d, me).start()

        rcv[c, tp, g] = snd[c, g]

    for copy in weights:
        copy.wait()

    osnd, back = (osnd0, osnd1, osnd2), (back0, back1, back2)
    zsnd, zrcv = (zsnd0, zsnd1, zsnd2), (zrcv0, zrcv1, zrcv2)
    units = [(0, 0, half), (1, 0, half // 2), (1, half // 2, half // 2)]

    def b_copy(u, d, at):
        q = lax.rem(me + d, np_)
        to_g, to_tp = q // 2, q % 2
        return remote(
            osnd[u].at[to_tp, to_g],
            back[u].at[at % 2, at // 2],
            b_sem.at[u],
            d,
            at,
            z * ng + to_g,
            to_tp,
        )

    for c in range(2):

        @pl.loop(1, np_)
        def _(d):
            d_copy(c, d, lax.rem(me + d, np_)).wait_recv()

        left = rcv[c, 0].reshape(ng * slots, half)
        right = rcv[c, 1].reshape(ng * slots, half)

        def both(w):
            return jnp.dot(left, w[:half, :], preferred_element_type=F32) + jnp.dot(
                right, w[half:, :], preferred_element_type=F32
            )

        gate_val = both(wg)
        hidden = (gate_val * jax.nn.sigmoid(gate_val) * both(wu)).astype(BF16)
        for u, (chunk, start, size) in enumerate(units):
            if chunk == c:
                for h in range(2):
                    cols = slice(h * half + start, h * half + start + size)
                    osnd[u][h] = (
                        jnp.dot(hidden, wd[:, cols], preferred_element_type=F32)
                        .astype(BF16)
                        .reshape(ng, slots, size)
                    )

                @pl.loop(1, np_)
                def _(d):
                    b_copy(u, d, me).start()

                back[u][tp, g] = osnd[u][tp, g]

    @pl.loop(1, np_)
    def _(d):
        for c in range(2):
            d_copy(c, d, me).wait_send()

    swap.wait_send()
    for o in range(1, nz):
        meta_out[o].wait_send()
        z_out[o].wait_send()

    summed = []
    for u, (c, start, size) in enumerate(units):
        r_out, _ = along_z(
            r_sem.at[u],
            lambda o: zsnd[u].at[o % per],
            lambda o: zrcv[u].at[o],
            range(max(1, c * per), (c + 1) * per),
        )

        @pl.loop(1, np_)
        def _(d):
            b_copy(u, d, lax.rem(me + d, np_)).wait_recv()

        served = (back[u][0].astype(F32) + back[u][1].astype(F32)).astype(BF16)
        served = served.reshape(ng * slots, size)
        mix_hi, mix_lo = mixes[c]
        sums = jnp.dot(mix_hi, served, preferred_element_type=F32) + jnp.dot(
            mix_lo, served, preferred_element_type=F32
        )
        for o in range(per):
            zsnd[u][o] = stacked(sums[o * rows : o * rows + count])
        for o in reversed(r_out):
            r_out[o].start()
            summed.append(r_out[o])

    @pl.loop(1, np_)
    def _(d):
        for u in range(3):
            b_copy(u, d, me).wait_send()

    total = my_half(resid).astype(F32) + unstacked(zsnd[0][0])
    def arrived(u):
        added = []
        for d in range(1, nz):
            if units[u][0] == place_of(nz - d, nz) // per:
                here = place_of(d, nz)
                at = zrcv[u].at[here]
                remote(at, at, r_sem.at[u], here, here, ep, other).wait_recv()
                added.append(unstacked(zrcv[u][here]))
        return sum(added[1:], added[0]) if added else 0.0

    total = total + arrived(0)
    lasts = []
    for f in range(2):
        _, start, size = units[1 + f]
        hbuf[0, f] = (total[:, start : start + size] + arrived(1 + f)).astype(BF16)
        lasts.append(remote(hbuf.at[0, f], hbuf.at[1, f], f_sem, f, f, ep, other))
        lasts[f].start()
    for f in range(2):
        _, start, size = units[1 + f]
        lasts[f].wait_recv()
        mine, theirs = hbuf[0, f], hbuf[1, f]
        out_ref[:, start : start + size] = jnp.where(tp == 0, mine, theirs)
        out_ref[:, half + start : half + start + size] = jnp.where(tp == 0, theirs, mine)

    for sent in summed:
        sent.wait_send()
    for last in lasts:
        last.wait_send()


def moe(nz, ng, gated, meta, wout, tok, gain, wg, wu, wd):
    count, width = tok.shape
    half = width // 2
    vmem = pl.BlockSpec(memory_space=pltpu.VMEM)
    hbm = pl.BlockSpec(memory_space=pltpu.HBM)

    sizes = (half, half // 2, half // 2)

    def sems(*n):
        return pltpu.SemaphoreType.DMA(n)

    return pl.pallas_call(
        functools.partial(moe_kernel, nz, ng),
        out_shape=pltpu.VMEM((count, width), BF16),
        in_specs=[vmem] * 2 + [hbm] * 6,
        out_specs=vmem,
        scratch_shapes=[pltpu.VMEM(a.shape, a.dtype) for a in (wout, tok, gain, wg, wu, wd)]
        + [
            pltpu.VMEM((2, count, width), BF16),
            pltpu.VMEM((nz, *meta.shape), F32),
            pltpu.VMEM((nz, 4 * count, half // 4), BF16),
            pltpu.VMEM((2, ng, nz, half), BF16),
            pltpu.VMEM((2, 2, ng, nz, half), BF16),
        ]
        + [pltpu.VMEM((2, ng, nz, n), BF16) for n in sizes] * 2
        + [pltpu.VMEM((nz // 2, 4 * count, n // 4), BF16) for n in sizes]
        + [pltpu.VMEM((nz, 4 * count, n // 4), BF16) for n in sizes]
        + [
            pltpu.VMEM((2, 2, count, half // 2), BF16),
            sems(6),
            sems(2, 1),
            sems(2, nz),
            sems(2, nz),
            sems(2, 2, 2 * ng),
            sems(3, 2, 2 * ng),
            sems(3, 2, nz),
            sems(2, 2),
        ],
        compiler_params=pltpu.CompilerParams(
            collective_id=0, has_side_effects=True, vmem_limit_bytes=MOST_VMEM
        ),
        name="experts",
    )(gated, meta, wout, tok, gain, wg, wu, wd)


def cell_kernel(
    tok_hbm,
    ngain_hbm,
    wi_hbm,
    wf_hbm,
    bias_hbm,
    hgain_hbm,
    norm_hbm,
    stab_hbm,
    ids_hbm,
    probs_hbm,
    wq_hbm,
    wk_hbm,
    wv_hbm,
    wo_hbm,
    mem_hbm,
    gated_ref,
    meta_ref,
    nnorm_hbm,
    nstab_hbm,
    nmem_hbm,
    tok_ref,
    ngain_ref,
    wi_ref,
    wf_ref,
    bias_ref,
    hgain_ref,
    norm_ref,
    stab_ref,
    ids_ref,
    probs_ref,
    wq,
    wk,
    wv,
    wo,
    mem,
    num,
    nnorm_ref,
    nstab_ref,
    o_sem,
    s_sem,
    w_sem,
    in_sem,
    out_sem,
):
    tp = lax.axis_index("tp")
    count, width = tok_ref.shape
    heads, dim = norm_ref.shape[1:]
    small = [
        pltpu.make_async_copy(src, dst, s_sem.at[i])
        for i, (src, dst) in enumerate(
            (
                (ids_hbm, ids_ref),
                (probs_hbm, probs_ref),
                (tok_hbm, tok_ref),
                (ngain_hbm, ngain_ref),
                (wi_hbm, wi_ref),
                (wf_hbm, wf_ref),
                (bias_hbm, bias_ref),
                (stab_hbm, stab_ref),
                (norm_hbm, norm_ref),
                (hgain_hbm, hgain_ref),
            )
        )
    ]
    loads = [
        pltpu.make_async_copy(src, dst, w_sem.at[i])
        for i, (src, dst) in enumerate(
            ((wk_hbm, wk), (wv_hbm, wv), (wq_hbm, wq), (wo_hbm, wo))
        )
    ]
    reads = [pltpu.make_async_copy(mem_hbm.at[b], mem.at[b], in_sem.at[b]) for b in range(count)]
    writes = [pltpu.make_async_copy(mem.at[b], nmem_hbm.at[b], out_sem.at[b]) for b in range(count)]
    third = count // 3
    for copy in small + loads[:3] + reads[:third]:
        copy.start()

    for copy in small:
        copy.wait()
    ids = ids_ref[...].astype(F32).T.astype(jnp.int32)
    probs = probs_ref[...].T
    weights = probs / jnp.sum(probs, axis=-1, keepdims=True)
    lane = lax.broadcasted_iota(jnp.int32, (count, 128), 1)
    row = lax.broadcasted_iota(jnp.int32, (count, 128), 0)
    top = ids.shape[1]
    named = [lane == ids[:, k : k + 1] for k in range(top)]
    onehot = jnp.zeros((count, 128), F32)
    for k in range(top):
        onehot = onehot + jnp.where(named[k], 1.0, 0.0)
    rows16 = meta_ref.shape[0] - 8
    lower = lax.broadcasted_iota(jnp.int32, (count, count), 0) > lax.broadcasted_iota(
        jnp.int32, (count, count), 1
    )
    earlier = jnp.dot(
        jnp.where(lower, 1.0, 0.0).astype(BF16), onehot.astype(BF16), preferred_element_type=F32
    )
    by_row = jnp.zeros((count, 128), F32)
    meta_ref[...] = jnp.zeros(meta_ref.shape, F32)
    for k in range(top):
        rank = jnp.sum(jnp.where(named[k], earlier, 0.0), axis=1, keepdims=True)
        code = ids[:, k : k + 1].astype(F32) + 1.0
        for at, what in ((k, code), (4 + k, weights[:, k : k + 1]), (8 + k, rank)):
            by_row = jnp.where(lane == at, what, by_row)
        for at, what in ((k, code), (4 + k, rank)):
            meta_ref[rows16 + at : rows16 + at + 1, :] = jnp.sum(
                jnp.where(lax.rem(lane, count) == row, what, 0.0), axis=0, keepdims=True
            )
    meta_ref[:count, :] = by_row

    normed = rms_scaled(tok_ref[...], ngain_ref[...]).astype(BF16)
    across = (((1,), (1,)), ((), ()))
    pre_all = lax.dot_general(normed, wi_ref[...], across, preferred_element_type=F32)
    forget_all = jax.nn.log_sigmoid(
        lax.dot_general(normed, wf_ref[...], across, preferred_element_type=F32) + bias_ref[...]
    )

    def project(i, w):
        loads[i].wait()
        return jnp.dot(normed, w[...], preferred_element_type=F32)

    key = project(0, wk) * dim ** (-0.5)
    for copy in reads[third : 2 * third]:
        copy.start()
    value = project(1, wv)
    for copy in reads[2 * third :] + loads[3:]:
        copy.start()
    query = project(2, wq)
    query_t = query.T
    stab = stab_ref[...].T
    new_stabs = []
    keeps, values, keys_t, floors = [], [], [], []
    for h in range(heads):
        pre = jnp.where(tp == 0, pre_all[:, h : h + 1], pre_all[:, heads + h : heads + h + 1])
        forget = jnp.where(
            tp == 0, forget_all[:, h : h + 1], forget_all[:, heads + h : heads + h + 1]
        )
        carried = forget + stab[:, h : h + 1]
        new_stab = jnp.maximum(carried, pre)
        new_stabs.append(new_stab)
        keep = jnp.exp(carried - new_stab)
        at = slice(h * dim, (h + 1) * dim)
        written = jnp.exp(pre - new_stab) * key[:, at]
        new_norm = keep * norm_ref[:, h, :] + written
        nnorm_ref[:, h, :] = new_norm
        den = jnp.sum(query[:, at] * new_norm, axis=1, keepdims=True)
        floors.append(jnp.maximum(jnp.abs(den), jnp.exp(-new_stab)))
        keeps.append(jnp.broadcast_to(keep, (count, dim)))
        key_hi = written.astype(BF16).astype(F32)
        value_hi = value[:, at].astype(BF16).astype(F32)
        keys_t.append(
            jnp.concatenate([key_hi, key_hi, written - key_hi], axis=0).T.astype(BF16)
        )
        values.append(jnp.concatenate([value_hi, value[:, at] - value_hi, value_hi], axis=0))
    heads_at = lax.broadcasted_iota(jnp.int32, (count, heads), 1)
    both_stabs = jnp.broadcast_to(new_stabs[0], (count, heads))
    for h in range(1, heads):
        both_stabs = jnp.where(heads_at == h, new_stabs[h], both_stabs)
    nstab_ref[...] = both_stabs.T
    results = [
        pltpu.make_async_copy(nnorm_ref, nnorm_hbm, o_sem.at[0]),
        pltpu.make_async_copy(nstab_ref, nstab_hbm, o_sem.at[1]),
    ]
    for copy in results:
        copy.start()
    sequence = lax.rem(lax.broadcasted_iota(jnp.int32, (3 * count, dim), 0), count)
    block = 96
    for b in range(count):
        reads[b].wait()
        for h in range(heads):
            kept = keeps[h][b : b + 1, :]
            added = jnp.where(sequence == b, values[h], 0.0).astype(BF16)
            folded = jnp.zeros((8, dim), F32)
            for d in range(0, dim, block):
                new = kept * mem[b, h, d : d + block, :] + jnp.dot(
                    keys_t[h][d : d + block, :], added, preferred_element_type=F32
                )
                mem[b, h, d : d + block, :] = new
                read = query_t[h * dim + d : h * dim + d + block, b : b + 1] * new
                folded = folded + jnp.sum(read.reshape(block // 8, 8, dim), axis=0)
            num[h, b : b + 1, :] = jnp.sum(folded, axis=0, keepdims=True)
        writes[b].start()
    outgate = project(3, wo)
    local_width = heads * dim
    parts = local_width // 128
    gains = jnp.concatenate(
        [
            jnp.where(tp == 0, hgain_ref[i : i + 1, :], hgain_ref[parts + i : parts + i + 1, :])
            for i in range(parts)
        ],
        axis=1,
    )
    for h in range(heads):
        at = slice(h * dim, (h + 1) * dim)
        readout = num[h] / floors[h]
        scaled = (
            readout
            * lax.rsqrt(jnp.mean(readout * readout, axis=-1, keepdims=True) + EPS)
            * gains[:, at]
        )
        gated_ref[:, at] = (scaled * jax.nn.sigmoid(outgate[:, at])).astype(BF16)
    for copy in writes + results:
        copy.wait()


def cell(small, weights, memory):
    count, width = small[0].shape
    rows16 = -(-count // 16) * 16
    norm_shape = small[6].shape
    vmem = pl.BlockSpec(memory_space=pltpu.VMEM)
    hbm = pl.BlockSpec(memory_space=pltpu.HBM)
    return pl.pallas_call(
        cell_kernel,
        out_shape=(
            pltpu.VMEM((count, weights[0].shape[1]), BF16),
            pltpu.VMEM((rows16 + 8, 128), F32),
            jax.ShapeDtypeStruct(norm_shape, F32),
            jax.ShapeDtypeStruct((norm_shape[1], count), F32),
            jax.ShapeDtypeStruct(memory.shape, F32),
        ),
        in_specs=[hbm] * (len(small) + len(weights) + 1),
        out_specs=(vmem, vmem, hbm, hbm, hbm),
        scratch_shapes=[pltpu.VMEM(a.shape, a.dtype) for a in (*small, *weights, memory)]
        + [
            pltpu.VMEM((norm_shape[1], count, norm_shape[2]), F32),
            pltpu.VMEM(norm_shape, F32),
            pltpu.VMEM((norm_shape[1], count), F32),
            pltpu.SemaphoreType.DMA((2,)),
            pltpu.SemaphoreType.DMA((len(small),)),
            pltpu.SemaphoreType.DMA((len(weights),)),
            pltpu.SemaphoreType.DMA((count,)),
            pltpu.SemaphoreType.DMA((count,)),
        ],
        compiler_params=pltpu.CompilerParams(vmem_limit_bytes=MOST_VMEM),
        name="cell",
    )(*small, *weights, memory)


def local(
    tokens,
    norm_gain,
    w_query,
    w_key,
    w_value,
    w_outgate,
    w_input_gate,
    w_forget_gate,
    forget_bias,
    head_gain,
    w_output,
    memory,
    normalizer,
    stabilizer,
    ffn_gain,
    route_ids,
    route_probs,
    expert_gate,
    expert_up,
    expert_down,
):
    ep_count = lax.axis_size("ep")
    ng = min(PLANE, ep_count // 2)
    nz = ep_count // ng
    gated, meta, new_normalizer, new_stab, new_memory = cell(
        (
            tokens,
            norm_gain.reshape(1, -1),
            w_input_gate.T,
            w_forget_gate.T,
            forget_bias.reshape(1, -1),
            head_gain.reshape(-1, 128),
            normalizer,
            stabilizer.T,
            route_ids.T,
            route_probs.T,
        ),
        (w_query, w_key, w_value, w_outgate),
        memory,
    )
    gated = pltpu.with_memory_space_constraint(gated, pltpu.VMEM)
    meta = pltpu.with_memory_space_constraint(meta, pltpu.VMEM)
    next_tokens = moe(
        nz,
        ng,
        gated,
        meta,
        w_output,
        tokens,
        ffn_gain.reshape(1, -1),
        expert_gate[0],
        expert_up[0],
        expert_down[0],
    )
    return (next_tokens, new_memory, new_normalizer, new_stab.T)


def solution(mesh):
    return jax.shard_map(
        local,
        mesh=mesh,
        in_specs=(
            P("ep", None),
            P(),
            P(None, "tp"),
            P(None, "tp"),
            P(None, "tp"),
            P(None, "tp"),
            P(),
            P(),
            P(),
            P(),
            P("tp", None),
            P("ep", "tp", None, None),
            P("ep", "tp", None),
            P("ep", "tp"),
            P(),
            P("ep", None),
            P("ep", None),
            P("ep", None, "tp"),
            P("ep", None, "tp"),
            P("ep", "tp", None),
        ),
        out_specs=(P("ep", None), P("ep", "tp", None, None), P("ep", "tp", None), P("ep", "tp")),
        check_vma=False,
    )
```
